512 devices in a mesh: ep: 128 (over z, x, core), tp: 4 (over y).
Axes of the slice: x: 4, y: 4, z: 16, core: 2. Of those that a mesh axis runs over, the one named last changes fastest.
Arguments:
- tokens: bfloat16 [2048, 1024], P('ep'), may hold values from -6 to 6
- state: float32 [2048, 16, 64, 64], P('ep', 'tp'), may hold values from -6 to 6
- w_recep: bfloat16 [1024, 1024], P(None, 'tp'), may hold values from -0.1875 to 0.1875
- w_key: bfloat16 [1024, 1024], P(None, 'tp'), may hold values from -0.1875 to 0.1875
- w_value: bfloat16 [1024, 1024], P(None, 'tp'), may hold values from -0.1875 to 0.1875
- w_out: bfloat16 [1024, 1024], P('tp'), may hold values from -0.1875 to 0.1875
- decay_base: float32 [1024], P('tp'), may hold values from -5 to 1
- decay_down: bfloat16 [1024, 64], replicated, may hold values from -0.1875 to 0.1875
- decay_up: bfloat16 [64, 1024], P(None, 'tp'), may hold values from -1 to 1
- rate_base: float32 [1024], P('tp'), may hold values from -4 to 4
- rate_down: bfloat16 [1024, 64], replicated, may hold values from -0.1875 to 0.1875
- rate_up: bfloat16 [64, 1024], P(None, 'tp'), may hold values from -1 to 1
- head_gain: float32 [1024], P('tp'), may hold values from 0.1 to 1.9
- first_gain: float32 [1024], replicated, may hold values from 0.2 to 4.8
- expert_gate: bfloat16 [128, 1024, 1408], P('ep', None, 'tp'), may hold values from -0.1875 to 0.1875
- expert_up: bfloat16 [128, 1024, 1408], P('ep', None, 'tp'), may hold values from -0.1875 to 0.1875
- expert_down: bfloat16 [128, 1408, 1024], P('ep', 'tp'), may hold values from -0.078125 to 0.078125
- dense_gate: bfloat16 [2816, 1024], P('ep'), may hold values from -0.1875 to 0.1875
- dense_up: bfloat16 [2816, 1024], P('ep'), may hold values from -0.1875 to 0.1875
- dense_down: bfloat16 [2816, 1024], P('ep', 'tp'), may hold values from -0.21875 to 0.21875
- branch_gate: bfloat16 [1024], replicated, may hold values from -0.1875 to 0.1875
- second_gain: float32 [1024], P('tp'), may hold values from 0.1 to 1.9
- routes: int32 [2048, 2], P('ep'), may hold values from 0 to 31, all different within a row; in each aligned block of 16 rows (0 to 15, 16 to 31, ...) at most 2 rows name the same one
- route_weights: float32 [2048, 2], P('ep'), may hold values from 0.2 to 1
Outputs:
- layer_output: bfloat16 [2048, 1024], P('ep', 'tp')
The draws below stay inside these ranges and needn't reach their ends.
Inputs may be any that keep to these rules, and one draw needn't show every extreme that they name: `routes`: each row names 2 different experts. In each aligned block of 16 rows no expert is named by more than 2 rows, a bound that some block reaches.
All inputs are finite; a program needn't handle non-finite values.
Results may differ from the reference program's by a relative error of at most 0.018.
Values may be sent and summed in bfloat16 or wider, within the bound.
No kernel may reach another device: no remote copies, remote signals or barrier semaphores. Data moves between devices by JAX's collectives and lax.ppermute only.
A program may use at most 64 MiB of HBM per device.

```python
import math
from functools import partial
import jax
import jax.numpy as jnp
import numpy as np
from jax import lax

MODEL_DIMENSION = 1024
HEAD = 64
RANK = 64
FF_E = 5632
FF_D = 2816
SPLIT = 4
TOP_K = 2
B_DEV = 16
HEADS = 16
TOKEN_TOTAL = 2048
EXPERTS = 32
CAP = 2
N_EP = 128


def draw_first_gain(key, part):
    position = jnp.arange(MODEL_DIMENSION, dtype=jnp.float32) / MODEL_DIMENSION
    jitter = jax.random.uniform(key, (MODEL_DIMENSION,), jnp.float32, 0.0, 1.0)
    return (0.5 + jitter) * jnp.exp(jnp.log(3.0) * position) * 0.6


def block_levels(rng, dims, shards, low, top_value):
    def one(dim, shards_of):
        draws = jax.random.uniform(jax.random.fold_in(jax.random.fold_in(rng, 6), dim), (shards_of,), jnp.float32, low / len(shards), top_value / len(shards))
        return jnp.repeat(jnp.exp(draws), dims[dim] // shards_of).reshape((-1,) + (1,) * (len(dims) - dim - 1))

    loudness = one(*shards[0])
    for cut in shards[1:]:
        loudness = loudness * one(*cut)
    return loudness


def shared_out(stream_key, own, number, rows, count, top, limit, skew):
    sequence = jax.random.permutation(stream_key, count)
    crowded, ordinary = load_shares(count, rows * top, limit, skew, True), load_shares(count, rows * top, limit, skew, False)
    places = jnp.arange(count)

    def named(lengths, turn):
        used = int((lengths > 0).sum())
        fixed = max(1, used // 4)
        passed = fixed + (places - fixed + turn * (used - fixed)) % max(1, count - fixed)
        return jnp.zeros((count,), jnp.int32).at[sequence[jnp.where(places < fixed, places, passed)]].set(jnp.asarray(lengths, jnp.int32))

    lengths = jnp.where(number % 4 == 0, named(crowded, number // 4), named(ordinary, number - number // 4 - 1))
    mixed = jax.random.permutation(jax.random.fold_in(own, 3), count)
    donor, taker = mixed[0:count // 2 * 2:2], mixed[1:count // 2 * 2:2]
    room = jnp.minimum(lengths[donor] - 1, limit - lengths[taker]) // 2
    room = jnp.where((donor == sequence[0]) | (taker == sequence[0]) | (lengths[taker] == 0), 0, jnp.maximum(room, 0))
    passed = jax.random.randint(jax.random.fold_in(own, 4), (count // 2,), 0, 1 << 20) % (room + 1)
    lengths = lengths.at[donor].add(-passed).at[taker].add(passed)
    items = jnp.searchsorted(jnp.cumsum(lengths), jnp.arange(rows * top), side="right").astype(jnp.int32)
    grid = items.reshape(top, rows).T
    grid = grid[jax.random.permutation(jax.random.fold_in(own, 1), rows)]
    turn = jax.random.randint(jax.random.fold_in(own, 2), (rows, 1), 0, top)
    return jnp.take_along_axis(grid, (jnp.arange(top)[None, :] + turn) % top, axis=1)


def load_shares(count, total, bound, slope, full):
    loads = [(1 << 20) // math.isqrt(rank ** slope) + 1 for rank in range(1, count + 1)]
    largest = bound if full else min(bound, max(-(-total // count), total * loads[0] // sum(loads)))
    least = 1 if total - largest >= count - 1 else 0
    holding, rest = [largest] + [least] * (count - 1), total - largest - least * (count - 1)
    while rest > 0:
        movable = [i for i in range(1, count) if holding[i] < largest] or [i for i in range(1, count) if holding[i] < bound]
        mass, left = sum([loads[i] for i in movable]), rest
        for i in movable:
            more = min(bound - holding[i], max(1, left * loads[i] // mass), rest)
            holding[i] = holding[i] + more
            rest = rest - more
    return np.array(holding)


def noise(key, shape, scale, reach, shards=(), held_as=jnp.bfloat16):
    values = jax.random.normal(key, shape, jnp.float32) * scale
    if len(shards) > 0:
        values = block_levels(key, shape, shards, -0.22, 0.18) * values
    return jnp.clip(values, min=-reach, max=reach).astype(held_as)


def setup_inputs(seed: int = 0) -> dict:
    key_list = jax.random.split(jax.random.key(seed), 25)
    tokens = noise(key_list[0], (TOKEN_TOTAL, MODEL_DIMENSION), 1.0, 6.0, ((0, 128),))
    state = noise(key_list[1], (TOKEN_TOTAL, HEADS, HEAD, HEAD), 1.0, 6.0, ((0, 128), (1, 4)), jnp.float32)
    w_recep = noise(key_list[2], (MODEL_DIMENSION, MODEL_DIMENSION), MODEL_DIMENSION ** -0.5, 0.1875, ((1, 4),))
    w_key = noise(key_list[3], (MODEL_DIMENSION, MODEL_DIMENSION), MODEL_DIMENSION ** -0.5, 0.1875, ((1, 4),))
    w_value = noise(key_list[4], (MODEL_DIMENSION, MODEL_DIMENSION), MODEL_DIMENSION ** -0.5, 0.1875, ((1, 4),))
    w_out = noise(key_list[5], (MODEL_DIMENSION, MODEL_DIMENSION), MODEL_DIMENSION ** -0.5, 0.1875, ((0, 4),))
    decay_base = jnp.clip(-5.0 + 6.0 * jax.random.uniform(key_list[6], (MODEL_DIMENSION,), jnp.float32) ** block_levels(key_list[6], (MODEL_DIMENSION,), ((0, 4),), -0.2, 0.2), -5.0, 1.0)
    decay_down = noise(key_list[7], (MODEL_DIMENSION, RANK), MODEL_DIMENSION ** -0.5, 0.1875)
    decay_up = noise(key_list[8], (RANK, MODEL_DIMENSION), (RANK // 2) ** -0.5, 1.0, ((1, 4),))
    rate_base = noise(key_list[9], (MODEL_DIMENSION,), 1.0, 4.0, ((0, 4),), jnp.float32)
    rate_down = noise(key_list[10], (MODEL_DIMENSION, RANK), MODEL_DIMENSION ** -0.5, 0.1875)
    rate_up = noise(key_list[11], (RANK, MODEL_DIMENSION), (RANK // 2) ** -0.5, 1.0, ((1, 4),))
    head_gain = jnp.clip(1.0 + 0.18 * jax.random.normal(key_list[12], (MODEL_DIMENSION,), jnp.float32), 0.1, 1.9)
    first_gain = draw_first_gain(jax.random.fold_in(key_list[24], 71), 0)
    expert_gate = noise(key_list[14], (N_EP, MODEL_DIMENSION, FF_E // SPLIT), MODEL_DIMENSION ** -0.5, 0.1875, ((0, 128), (2, 4)))
    expert_up = noise(key_list[15], (N_EP, MODEL_DIMENSION, FF_E // SPLIT), MODEL_DIMENSION ** -0.5, 0.1875, ((0, 128), (2, 4)))
    expert_down = noise(key_list[16], (N_EP, FF_E // SPLIT, MODEL_DIMENSION), FF_E ** -0.5, 0.078125, ((0, 128), (1, 4)))
    dense_gate = noise(key_list[17], (FF_D, MODEL_DIMENSION), MODEL_DIMENSION ** -0.5, 0.1875, ((0, 128),))
    dense_up = noise(key_list[18], (FF_D, MODEL_DIMENSION), MODEL_DIMENSION ** -0.5, 0.1875, ((0, 128),))
    dense_down = noise(key_list[19], (FF_D, MODEL_DIMENSION), (FF_D // 4) ** -0.5, 0.21875, ((0, 128), (1, 4)))
    branch_gate = noise(key_list[20], (MODEL_DIMENSION,), MODEL_DIMENSION ** -0.5, 0.1875)
    second_gain = jnp.clip(1.0 + 0.18 * jax.random.normal(key_list[21], (MODEL_DIMENSION,), jnp.float32), 0.1, 1.9)
    routes_keys = jax.random.split(jax.random.fold_in(key_list[22], 1), TOKEN_TOTAL // B_DEV)
    routes_turns = jax.random.permutation(jax.random.fold_in(key_list[22], 3), TOKEN_TOTAL // B_DEV)
    routes = jax.vmap(lambda own, number: shared_out(jax.random.fold_in(key_list[22], 2), own, number, B_DEV, EXPERTS, TOP_K, CAP, 2))(routes_keys, routes_turns).reshape((TOKEN_TOTAL, TOP_K))
    route_weights = jnp.clip(0.2 + 0.8 * jax.random.uniform(key_list[23], (TOKEN_TOTAL, TOP_K), jnp.float32) ** block_levels(key_list[23], (TOKEN_TOTAL, TOP_K), ((0, 128),), -0.2, 0.2), 0.2, 1.0)
    return dict(tokens=tokens, state=state, w_recep=w_recep, w_key=w_key, w_value=w_value, w_out=w_out, decay_base=decay_base, decay_down=decay_down, decay_up=decay_up, rate_base=rate_base, rate_down=rate_down, rate_up=rate_up, head_gain=head_gain, first_gain=first_gain, expert_gate=expert_gate, expert_up=expert_up, expert_down=expert_down, dense_gate=dense_gate, dense_up=dense_up, dense_down=dense_down, branch_gate=branch_gate, second_gain=second_gain, routes=routes, route_weights=route_weights)


residual_scale = 1.4142135623730951
norm_epsilon = 1e-05
head_epsilon = 0.00064
key_epsilon = 1e-06

def time_mixer(tokens, state, w_recep, w_key, w_value, w_out, decay_base, decay_down, decay_up, rate_base, rate_down, rate_up, head_gain):
    row_count = tokens.shape[0]
    head_count = state.shape[1]
    head_size = state.shape[3]
    recep = jnp.dot(tokens, w_recep, preferred_element_type=jnp.float32).reshape(row_count, head_count, head_size)
    key_vecs = jnp.dot(tokens, w_key, preferred_element_type=jnp.float32).reshape(row_count, head_count, head_size)
    value_vecs = jnp.dot(tokens, w_value, preferred_element_type=jnp.float32).reshape(row_count, head_count, head_size)
    decay_low = jnp.tanh(jnp.dot(tokens, decay_down, preferred_element_type=jnp.float32)).astype(jnp.bfloat16)
    decay_pre = decay_base + jnp.dot(decay_low, decay_up, preferred_element_type=jnp.float32)
    log_rate = -jax.nn.softplus(-decay_pre) - 0.5
    decay = jnp.exp(-jnp.exp(log_rate)).reshape(row_count, head_count, head_size)
    rate_low = jnp.dot(tokens, rate_down, preferred_element_type=jnp.float32).astype(jnp.bfloat16)
    in_rate = jax.nn.sigmoid(rate_base + jnp.dot(rate_low, rate_up, preferred_element_type=jnp.float32)).reshape(row_count, head_count, head_size)
    unit_keys = key_vecs * lax.rsqrt(lax.optimization_barrier(jnp.sum(key_vecs * key_vecs, -1, keepdims=True)) + key_epsilon)
    removed = jnp.einsum('bhij,bhj->bhi', state, -unit_keys)
    updated = state * decay[:, :, None, :] + removed[..., None] * (unit_keys * in_rate)[:, :, None, :] + value_vecs[..., None] * key_vecs[:, :, None, :]
    read_out = jnp.einsum('bhij,bhj->bhi', updated, recep)
    centre = lax.optimization_barrier(jnp.mean(read_out, -1, keepdims=True))
    spread = lax.optimization_barrier(jnp.mean(jnp.square(read_out - centre), -1, keepdims=True))
    normed = ((read_out - centre) * lax.rsqrt(spread + head_epsilon)).reshape(row_count, head_count * head_size) * head_gain
    return jnp.dot(normed.astype(jnp.bfloat16), w_out, preferred_element_type=jnp.float32)

def first_norm(values, gain):
    centre = lax.optimization_barrier(jnp.mean(values, -1, keepdims=True))
    spread = lax.optimization_barrier(jnp.mean(jnp.square(values - centre), -1, keepdims=True))
    return ((values - centre) * lax.rsqrt(spread + norm_epsilon) * gain).astype(jnp.bfloat16)

def route_tables(routes, route_weights, experts, capacity):
    expert_hits = (routes[:, :, None] == jnp.arange(experts, dtype=jnp.int32)[None, None, :]).astype(jnp.int32)
    row_hits = lax.optimization_barrier(jnp.sum(expert_hits, 1, dtype=jnp.int32))
    earlier = jnp.cumsum(row_hits, 0, dtype=jnp.int32) - row_hits
    slot_index = lax.optimization_barrier(jnp.sum(earlier[:, None, :] * expert_hits, 2, dtype=jnp.int32))
    target = routes * capacity + slot_index
    places = jnp.arange(experts * capacity, dtype=jnp.int32)
    slot_match = target[:, :, None] == places[None, None, :]
    dispatch_tokens = jnp.any(slot_match, 1).astype(jnp.bfloat16)
    combine_experts = lax.optimization_barrier(jnp.sum(jnp.where(slot_match, route_weights[:, :, None], 0.0), 1))
    return (dispatch_tokens, combine_experts)

def one_expert(operands):
    rows_in, gate_all, up_all, down_all = operands
    gate_pre = jnp.dot(rows_in, gate_all, preferred_element_type=jnp.float32)
    up_pre = jnp.dot(rows_in, up_all, preferred_element_type=jnp.float32)
    hidden = (jax.nn.silu(gate_pre) * up_pre).astype(jnp.bfloat16)
    return jnp.dot(hidden, down_all, preferred_element_type=jnp.float32)

def reference(tokens, state, w_recep, w_key, w_value, w_out, decay_base, decay_down, decay_up, rate_base, rate_down, rate_up, head_gain, first_gain, expert_gate, expert_up, expert_down, dense_gate, dense_up, dense_down, branch_gate, second_gain, routes, route_weights):
    mixed = time_mixer(tokens, state, w_recep, w_key, w_value, w_out, decay_base, decay_down, decay_up, rate_base, rate_down, rate_up, head_gain)
    x_mid = first_norm(residual_scale * tokens.astype(jnp.float32) + mixed, first_gain)
    route_blocks = routes.reshape(N_EP, B_DEV, TOP_K)
    weight_blocks = route_weights.reshape(N_EP, B_DEV, TOP_K)
    dispatch_tokens, combine_experts = jax.vmap(partial(route_tables, experts=EXPERTS, capacity=CAP))(route_blocks, weight_blocks)
    token_block_rows = x_mid.reshape(N_EP, B_DEV, MODEL_DIMENSION).astype(jnp.float32)
    packed_rows = jnp.einsum('ekc,ekq->ecq', dispatch_tokens.astype(jnp.float32), token_block_rows).astype(jnp.bfloat16)
    expert_rows = packed_rows.reshape(N_EP, EXPERTS, CAP, MODEL_DIMENSION).transpose(1, 0, 2, 3).reshape(EXPERTS, N_EP * CAP, MODEL_DIMENSION)
    gate_all = expert_gate.reshape(EXPERTS, SPLIT, MODEL_DIMENSION, FF_E // SPLIT).transpose(0, 2, 1, 3).reshape(EXPERTS, MODEL_DIMENSION, FF_E)
    up_all = expert_up.reshape(EXPERTS, SPLIT, MODEL_DIMENSION, FF_E // SPLIT).transpose(0, 2, 1, 3).reshape(EXPERTS, MODEL_DIMENSION, FF_E)
    down_all = expert_down.reshape(EXPERTS, FF_E, MODEL_DIMENSION)
    produced = lax.map(one_expert, (expert_rows, gate_all, up_all, down_all))
    returned_rows = produced.reshape(EXPERTS, N_EP, CAP, MODEL_DIMENSION).transpose(1, 0, 2, 3).reshape(N_EP, EXPERTS * CAP, MODEL_DIMENSION)
    routed_tokens = jnp.einsum('lhs,lsu->lhu', combine_experts, returned_rows, precision=lax.Precision.HIGHEST).reshape(TOKEN_TOTAL, MODEL_DIMENSION)
    gate_pre = lax.dot_general(x_mid, dense_gate, (((1,), (1,)), ((), ())), preferred_element_type=jnp.float32)
    up_pre = lax.dot_general(x_mid, dense_up, (((1,), (1,)), ((), ())), preferred_element_type=jnp.float32)
    dense_hidden = (jax.nn.silu(gate_pre) * up_pre).astype(jnp.bfloat16)
    dense_part = jnp.dot(dense_hidden, dense_down, preferred_element_type=jnp.float32)
    branch = jax.nn.sigmoid(jnp.dot(x_mid, branch_gate, preferred_element_type=jnp.float32))
    second_sum = residual_scale * x_mid.astype(jnp.float32) + routed_tokens + branch[:, None] * dense_part
    average = lax.optimization_barrier(jnp.mean(second_sum, 1))
    square_mean = lax.optimization_barrier(jnp.mean(second_sum * second_sum, 1))
    spread = square_mean - average * average
    return ((second_sum - average[:, None]) * lax.rsqrt(spread + norm_epsilon)[:, None] * second_gain).astype(jnp.bfloat16)
```

```python
import jax
import jax.numpy as jnp
from jax import lax
from jax.sharding import Mesh
from jax.sharding import PartitionSpec as P

SPLIT = 4
EP = ("z", "x", "c")
PLANE = ("x", "c", "tp")


residual_scale = 1.4142135623730951
norm_epsilon = 1e-05
head_epsilon = 0.00064
key_epsilon = 1e-06


def sent_to_all(value, axis):
    copies = jnp.broadcast_to(value, (lax.axis_size(axis), *value.shape))
    return lax.all_to_all(copies, axis, split_axis=0, concat_axis=0, tiled=True)


def of_everyone(value, axis):
    return sent_to_all(value, axis).astype(jnp.float32).sum(axis=0)


def exchange(parts, axis):
    return lax.all_to_all(parts, axis, split_axis=0, concat_axis=0, tiled=True)


def in_one(arrays, axis):
    vector, at, done = (jnp.concatenate([a.reshape(-1) for a in arrays]), 0, [])
    running = of_everyone(vector, axis)
    for a in arrays:
        done.append(running[at : at + a.size].reshape(a.shape))
        at += a.size
    return tuple(done)


def plane_weights(dense_gate, dense_up, dense_down, quarter):
    y = lax.axis_size("tp")
    z = lax.axis_size("z")
    tp_index = lax.axis_index("tp")
    gate = lax.dynamic_slice_in_dim(dense_gate, tp_index * quarter, quarter, 1)
    up = lax.dynamic_slice_in_dim(dense_up, tp_index * quarter, quarter, 1)
    units = gate.shape[0]
    part = -(-units // y)
    three = jnp.stack([gate, up, dense_down])
    three = jnp.pad(three, ((0, 0), (0, part * y - units), (0, 0)))
    three = three.reshape(3, y, part, quarter).swapaxes(0, 1)
    message = three.reshape(y, 3 * part * quarter // 128, 128)
    outgoing = jnp.broadcast_to(message, (z, *message.shape)).reshape(z * y, *message.shape[1:])
    arrived = exchange(outgoing, ("z", "tp"))
    arrived = arrived.reshape(z, y, 3, part, quarter)
    return arrived.transpose(2, 0, 3, 1, 4).reshape(3, z * part, y * quarter)


def time_mixer(
    tokens,
    state,
    w_recep,
    w_key,
    w_value,
    w_out,
    decay_base,
    decay_down,
    decay_up,
    rate_base,
    rate_down,
    rate_up,
    head_gain,
):
    row_count = tokens.shape[0]
    head_count = state.shape[1]
    head_size = state.shape[3]
    recep = jnp.dot(tokens, w_recep, preferred_element_type=jnp.float32).reshape(
        row_count, head_count, head_size
    )
    key_vecs = jnp.dot(tokens, w_key, preferred_element_type=jnp.float32).reshape(
        row_count, head_count, head_size
    )
    value_vecs = jnp.dot(tokens, w_value, preferred_element_type=jnp.float32).reshape(
        row_count, head_count, head_size
    )
    decay_low = jnp.tanh(jnp.dot(tokens, decay_down, preferred_element_type=jnp.float32)).astype(
        jnp.bfloat16
    )
    decay_pre = decay_base + jnp.dot(decay_low, decay_up, preferred_element_type=jnp.float32)
    log_rate = -jax.nn.softplus(-decay_pre) - 0.5
    decay = jnp.exp(-jnp.exp(log_rate)).reshape(row_count, head_count, head_size)
    rate_low = jnp.dot(tokens, rate_down, preferred_element_type=jnp.float32).astype(jnp.bfloat16)
    in_rate = jax.nn.sigmoid(
        rate_base + jnp.dot(rate_low, rate_up, preferred_element_type=jnp.float32)
    ).reshape(row_count, head_count, head_size)
    unit_keys = key_vecs * lax.rsqrt(jnp.sum(key_vecs * key_vecs, -1, keepdims=True) + key_epsilon)
    removed = jnp.einsum("bhij,bhj->bhi", state, -unit_keys)
    updated = (
        state * decay[:, :, None, :]
        + removed[..., None] * (unit_keys * in_rate)[:, :, None, :]
        + value_vecs[..., None] * key_vecs[:, :, None, :]
    )
    read_out = jnp.einsum("bhij,bhj->bhi", updated, recep)
    centre = jnp.mean(read_out, -1, keepdims=True)
    spread = jnp.mean(jnp.square(read_out - centre), -1, keepdims=True)
    normed = ((read_out - centre) * lax.rsqrt(spread + head_epsilon)).reshape(
        row_count, head_count * head_size
    ) * head_gain
    return jnp.dot(normed.astype(jnp.bfloat16), w_out, preferred_element_type=jnp.float32)


def first_norm(values, gain):
    centre = jnp.mean(values, -1, keepdims=True)
    spread = jnp.mean(jnp.square(values - centre), -1, keepdims=True)
    return ((values - centre) * lax.rsqrt(spread + norm_epsilon) * gain).astype(jnp.bfloat16)


def route_tables(routes, route_weights, experts, capacity):
    expert_hits = (
        routes[:, :, None] == jnp.arange(experts, dtype=jnp.int32)[None, None, :]
    ).astype(jnp.int32)
    row_hits = jnp.sum(expert_hits, 1, dtype=jnp.int32)
    earlier = jnp.cumsum(row_hits, 0, dtype=jnp.int32) - row_hits
    slot_index = jnp.sum(earlier[:, None, :] * expert_hits, 2, dtype=jnp.int32)
    target = routes * capacity + slot_index
    places = jnp.arange(experts * capacity, dtype=jnp.int32)
    slot_match = target[:, :, None] == places[None, None, :]
    dispatch_tokens = jnp.any(slot_match, 1).astype(jnp.bfloat16)
    combine_experts = jnp.sum(jnp.where(slot_match, route_weights[:, :, None], 0.0), 1)
    return (dispatch_tokens, combine_experts)


def shards(
    tokens,
    state,
    w_recep,
    w_key,
    w_value,
    w_out,
    decay_base,
    decay_down,
    decay_up,
    rate_base,
    rate_down,
    rate_up,
    head_gain,
    first_gain,
    expert_gate,
    expert_up,
    expert_down,
    dense_gate,
    dense_up,
    dense_down,
    branch_gate,
    second_gain,
    routes,
    route_weights,
):
    row_count = tokens.shape[0]
    model_width = tokens.shape[1]
    quarter = w_recep.shape[1]
    tp_index = lax.axis_index("tp")
    planes = lax.axis_size("z")
    plane_blocks = lax.axis_size(("x", "c"))
    plane_size = lax.axis_size(PLANE)
    tp_size = lax.axis_size("tp")
    weights = plane_weights(dense_gate, dense_up, dense_down, quarter)
    partial_mix = time_mixer(
        tokens,
        state,
        w_recep,
        w_key,
        w_value,
        w_out,
        decay_base,
        decay_down,
        decay_up,
        rate_base,
        rate_down,
        rate_up,
        head_gain,
    )
    mixed = of_everyone(partial_mix.astype(jnp.bfloat16), "tp")
    x_mid = first_norm(residual_scale * tokens.astype(jnp.float32) + mixed, first_gain)
    own_columns = lax.dynamic_slice_in_dim(x_mid, tp_index * quarter, quarter, 1)
    experts = lax.axis_size(EP) // SPLIT
    here = experts // planes
    capacity = min(row_count, max(2, 2 * row_count * routes.shape[1] // experts))
    dispatch_tokens, combine_experts = route_tables(routes, route_weights, experts, capacity)
    packed_rows = lax.dot_general(
        dispatch_tokens, own_columns, (((0,), (0,)), ((), ())), preferred_element_type=jnp.float32
    ).astype(jnp.bfloat16)
    arrived = exchange(packed_rows.reshape(planes, here * capacity, quarter), "z")
    rows = planes * capacity
    arrived = arrived.reshape(planes, here, capacity, quarter).swapaxes(0, 1)
    arrived = arrived.reshape(here, rows, quarter)
    both = jnp.concatenate([arrived, jnp.broadcast_to(own_columns, (here, *own_columns.shape))], 1)
    outgoing = jnp.repeat(both, plane_size // here, axis=0)
    everything = exchange(outgoing, PLANE)
    everything = everything.reshape(plane_blocks, tp_size, rows + row_count, quarter).swapaxes(1, 2)
    everything = everything.reshape(plane_blocks, rows + row_count, model_width)
    flat_rows = everything[:, :rows].reshape(plane_blocks * rows, model_width)
    dense_rows = everything[:, rows:].reshape(plane_blocks * row_count, model_width)
    gate_pre = jnp.dot(flat_rows, expert_gate[0], preferred_element_type=jnp.float32)
    up_pre = jnp.dot(flat_rows, expert_up[0], preferred_element_type=jnp.float32)
    hidden = (jax.nn.silu(gate_pre) * up_pre).astype(jnp.bfloat16)
    partial_out = jnp.dot(hidden, expert_down[0], preferred_element_type=jnp.float32)
    dense_pre = [
        lax.dot_general(
            dense_rows, weights[i], (((1,), (1,)), ((), ())), preferred_element_type=jnp.float32
        )
        for i in range(2)
    ]
    dense_hidden = (jax.nn.silu(dense_pre[0]) * dense_pre[1]).astype(jnp.bfloat16)
    dense_out = jnp.dot(dense_hidden, weights[2], preferred_element_type=jnp.float32)
    returning = jnp.concatenate(
        [
            partial_out.astype(jnp.bfloat16).reshape(plane_blocks, rows, model_width),
            dense_out.astype(jnp.bfloat16).reshape(plane_blocks, row_count, model_width),
        ],
        1,
    )
    returning = returning.reshape(plane_blocks, rows + row_count, tp_size, quarter).swapaxes(1, 2)
    returned = exchange(returning.reshape(plane_size, rows + row_count, quarter), PLANE)
    returned = returned.astype(jnp.float32)
    dense_part = jnp.sum(returned[:, rows:], 0)
    summed = jnp.sum(returned[:, :rows].reshape(here, plane_size // here, rows, quarter), 1)
    summed = summed.reshape(here, planes, capacity, quarter).swapaxes(0, 1).astype(jnp.bfloat16)
    expert_out = exchange(summed.reshape(planes, here * capacity, quarter), "z")
    expert_out = expert_out.reshape(experts * capacity, quarter).astype(jnp.float32)
    routed_part = jnp.dot(
        combine_experts,
        expert_out,
        precision=lax.Precision.HIGHEST,
        preferred_element_type=jnp.float32,
    )
    branch = jax.nn.sigmoid(jnp.dot(x_mid, branch_gate, preferred_element_type=jnp.float32))
    second_sum = (
        residual_scale * own_columns.astype(jnp.float32)
        + routed_part
        + branch[:, None] * dense_part
    )
    row_sums, square_sums = in_one(
        (jnp.sum(second_sum, 1), jnp.sum(second_sum * second_sum, 1)), "tp"
    )
    average = row_sums / model_width
    spread = square_sums / model_width - average * average
    return (
        (second_sum - average[:, None]) * lax.rsqrt(spread + norm_epsilon)[:, None] * second_gain
    ).astype(jnp.bfloat16)


def solution(mesh):
    finer = Mesh(mesh.devices.reshape(16, 4, 2, mesh.shape["tp"]), ("z", "x", "c", "tp"))
    return jax.shard_map(
        shards,
        mesh=finer,
        in_specs=(
            P(EP, None),
            P(EP, "tp", None, None),
            P(None, "tp"),
            P(None, "tp"),
            P(None, "tp"),
            P("tp", None),
            P("tp"),
            P(),
            P(None, "tp"),
            P("tp"),
            P(),
            P(None, "tp"),
            P("tp"),
            P(),
            P(EP, None, "tp"),
            P(EP, None, "tp"),
            P(EP, "tp", None),
            P(EP, None),
            P(EP, None),
            P(EP, "tp"),
            P(),
            P("tp"),
            P(EP, None),
            P(EP, None),
        ),
        out_specs=P(EP, "tp"),
        check_vma=False,
    )
```

```python
import jax
import jax.numpy as jnp
from jax import lax
from jax.sharding import Mesh
from jax.sharding import PartitionSpec as P

SPLIT = 4
EP = ("z", "x", "c")
PLANE = ("x", "c", "tp")


residual_scale = 1.4142135623730951
norm_epsilon = 1e-05
head_epsilon = 0.00064
key_epsilon = 1e-06


def sent_to_all(value, axis):
    copies = jnp.broadcast_to(value, (lax.axis_size(axis), *value.shape))
    return lax.all_to_all(copies, axis, split_axis=0, concat_axis=0, tiled=True)


def of_everyone(value, axis):
    return sent_to_all(value, axis).astype(jnp.float32).sum(axis=0)


def exchange(parts, axis):
    return lax.all_to_all(parts, axis, split_axis=0, concat_axis=0, tiled=True)


def in_one(arrays, axis):
    vector, at, done = (jnp.concatenate([a.reshape(-1) for a in arrays]), 0, [])
    running = of_everyone(vector, axis)
    for a in arrays:
        done.append(running[at : at + a.size].reshape(a.shape))
        at += a.size
    return tuple(done)


def padded_units(columns, multiple):
    return jnp.pad(columns, ((0, -columns.shape[0] % multiple), (0, 0)))


def with_neighbour(units, step):
    planes = lax.axis_size("z")
    other = lax.ppermute(units, "z", [(i, i ^ step) for i in range(planes)])
    return jnp.concatenate([units, other], 0)


def time_mixer(
    tokens,
    state,
    w_recep,
    w_key,
    w_value,
    w_out,
    decay_base,
    decay_down,
    decay_up,
    rate_base,
    rate_down,
    rate_up,
    head_gain,
):
    row_count = tokens.shape[0]
    head_count = state.shape[1]
    head_size = state.shape[3]
    recep = jnp.dot(tokens, w_recep, preferred_element_type=jnp.float32).reshape(
        row_count, head_count, head_size
    )
    key_vecs = jnp.dot(tokens, w_key, preferred_element_type=jnp.float32).reshape(
        row_count, head_count, head_size
    )
    value_vecs = jnp.dot(tokens, w_value, preferred_element_type=jnp.float32).reshape(
        row_count, head_count, head_size
    )
    decay_low = jnp.tanh(jnp.dot(tokens, decay_down, preferred_element_type=jnp.float32)).astype(
        jnp.bfloat16
    )
    decay_pre = decay_base + jnp.dot(decay_low, decay_up, preferred_element_type=jnp.float32)
    log_rate = -jax.nn.softplus(-decay_pre) - 0.5
    decay = jnp.exp(-jnp.exp(log_rate)).reshape(row_count, head_count, head_size)
    rate_low = jnp.dot(tokens, rate_down, preferred_element_type=jnp.float32).astype(jnp.bfloat16)
    in_rate = jax.nn.sigmoid(
        rate_base + jnp.dot(rate_low, rate_up, preferred_element_type=jnp.float32)
    ).reshape(row_count, head_count, head_size)
    unit_keys = key_vecs * lax.rsqrt(jnp.sum(key_vecs * key_vecs, -1, keepdims=True) + key_epsilon)
    removed = jnp.einsum("bhij,bhj->bhi", state, -unit_keys)
    updated = (
        state * decay[:, :, None, :]
        + removed[..., None] * (unit_keys * in_rate)[:, :, None, :]
        + value_vecs[..., None] * key_vecs[:, :, None, :]
    )
    read_out = jnp.einsum("bhij,bhj->bhi", updated, recep)
    centre = jnp.mean(read_out, -1, keepdims=True)
    spread = jnp.mean(jnp.square(read_out - centre), -1, keepdims=True)
    normed = ((read_out - centre) * lax.rsqrt(spread + head_epsilon)).reshape(
        row_count, head_count * head_size
    ) * head_gain
    return jnp.dot(normed.astype(jnp.bfloat16), w_out, preferred_element_type=jnp.float32)


def first_norm(values, gain):
    centre = jnp.mean(values, -1, keepdims=True)
    spread = jnp.mean(jnp.square(values - centre), -1, keepdims=True)
    return ((values - centre) * lax.rsqrt(spread + norm_epsilon) * gain).astype(jnp.bfloat16)


def route_targets(routes, experts, capacity):
    expert_hits = (
        routes[:, :, None] == jnp.arange(experts, dtype=jnp.int32)[None, None, :]
    ).astype(jnp.int32)
    row_hits = jnp.sum(expert_hits, 1, dtype=jnp.int32)
    earlier = jnp.cumsum(row_hits, 0, dtype=jnp.int32) - row_hits
    slot_index = jnp.sum(earlier[:, None, :] * expert_hits, 2, dtype=jnp.int32)
    return routes * capacity + slot_index


def shards(
    tokens,
    state,
    w_recep,
    w_key,
    w_value,
    w_out,
    decay_base,
    decay_down,
    decay_up,
    rate_base,
    rate_down,
    rate_up,
    head_gain,
    first_gain,
    expert_gate,
    expert_up,
    expert_down,
    dense_gate,
    dense_up,
    dense_down,
    branch_gate,
    second_gain,
    routes,
    route_weights,
):
    row_count = tokens.shape[0]
    model_width = tokens.shape[1]
    quarter = w_recep.shape[1]
    tp_index = lax.axis_index("tp")
    planes = lax.axis_size("z")
    plane_blocks = lax.axis_size(("x", "c"))
    plane_size = lax.axis_size(PLANE)
    tp_size = lax.axis_size("tp")
    shared = planes // tp_size
    own_down = padded_units(dense_down, 8)
    partial_mix = time_mixer(
        tokens,
        state,
        w_recep,
        w_key,
        w_value,
        w_out,
        decay_base,
        decay_down,
        decay_up,
        rate_base,
        rate_down,
        rate_up,
        head_gain,
    ).astype(jnp.bfloat16)
    message = jnp.concatenate(
        [partial_mix[:, i * quarter : (i + 1) * quarter] for i in range(tp_size)]
        + [own_down],
        0,
    )
    everyone = sent_to_all(message, "tp")
    mix_rows = tp_size * row_count
    mixed = jnp.sum(everyone[:, :mix_rows].astype(jnp.float32), 0)
    mixed = jnp.concatenate(
        [mixed[i * row_count : (i + 1) * row_count] for i in range(tp_size)], 1
    )
    units = jnp.concatenate(
        [padded_units(dense_gate, 8), padded_units(dense_up, 8)]
        + [everyone[i, mix_rows:] for i in range(tp_size)],
        1,
    )
    units = with_neighbour(units, 1)
    x_mid = first_norm(residual_scale * tokens.astype(jnp.float32) + mixed, first_gain)
    own_columns = lax.dynamic_slice_in_dim(x_mid, tp_index * quarter, quarter, 1)
    experts = lax.axis_size(EP) // SPLIT
    here = experts // planes
    capacity = min(row_count, max(2, 2 * row_count * routes.shape[1] // experts))
    slots = here * capacity
    part = row_count // shared
    target = route_targets(routes, experts, capacity)
    place = jnp.arange(planes * (slots + part), dtype=jnp.int32)
    plane, inner = place // (slots + part), place % (slots + part)
    routed_place = jnp.where(inner < slots, plane * slots + inner, -1)
    dense_place = jnp.where(inner < slots, -1, plane % shared * part + inner - slots)
    slot_match = target[:, :, None] == routed_place[None, None, :]
    row_match = jnp.arange(row_count, dtype=jnp.int32)[:, None] == dense_place[None, :]
    chosen = (jnp.any(slot_match, 1) | row_match).astype(jnp.bfloat16)
    packed_rows = lax.dot_general(
        chosen, own_columns, (((0,), (0,)), ((), ())), preferred_element_type=jnp.float32
    ).astype(jnp.bfloat16)
    arrived = exchange(packed_rows.reshape(planes, slots + part, quarter), "z")
    arrived, units = lax.optimization_barrier((arrived, units))
    units = with_neighbour(units, 2)
    rows = planes * capacity
    dense_count = shared * part
    height = rows + dense_count
    routed_rows = arrived[:, :slots].reshape(planes, here, capacity, quarter).swapaxes(0, 1)
    routed_rows = routed_rows.reshape(here, 1, 1, rows, quarter)
    dense_rows = arrived[:, slots:].reshape(1, 1, tp_size, dense_count, quarter)
    wide = (here, plane_blocks // here, tp_size)
    outgoing = jnp.concatenate(
        [
            jnp.broadcast_to(routed_rows, (*wide, rows, quarter)),
            jnp.broadcast_to(dense_rows, (*wide, dense_count, quarter)),
        ],
        3,
    )
    everything = exchange(outgoing.reshape(plane_size, height, quarter), PLANE)
    everything = everything.reshape(plane_blocks, tp_size, height, quarter).swapaxes(1, 2)
    everything = everything.reshape(plane_blocks, height, model_width)
    flat_rows = everything[:, :rows].reshape(plane_blocks * rows, model_width)
    dense_rows = everything[:, rows:].reshape(plane_blocks * dense_count, model_width)
    gate_pre = jnp.dot(flat_rows, expert_gate[0], preferred_element_type=jnp.float32)
    up_pre = jnp.dot(flat_rows, expert_up[0], preferred_element_type=jnp.float32)
    hidden = (jax.nn.silu(gate_pre) * up_pre).astype(jnp.bfloat16)
    partial_out = jnp.dot(hidden, expert_down[0], preferred_element_type=jnp.float32)
    dense_pre = [
        lax.dot_general(
            dense_rows,
            units[:, i * model_width : (i + 1) * model_width],
            (((1,), (1,)), ((), ())),
            preferred_element_type=jnp.float32,
        )
        for i in range(2)
    ]
    dense_hidden = (jax.nn.silu(dense_pre[0]) * dense_pre[1]).astype(jnp.bfloat16)
    partial_out = partial_out.astype(jnp.bfloat16)
    returning = jnp.stack(
        [
            jnp.concatenate(
                [
                    partial_out[:, i * quarter : (i + 1) * quarter].reshape(
                        plane_blocks, rows, quarter
                    ),
                    jnp.dot(
                        dense_hidden,
                        units[:, 2 * model_width + i * quarter :][:, :quarter],
                        preferred_element_type=jnp.float32,
                    )
                    .astype(jnp.bfloat16)
                    .reshape(plane_blocks, dense_count, quarter),
                ],
                1,
            )
            for i in range(tp_size)
        ],
        1,
    )
    returned = exchange(returning.reshape(plane_size, height, quarter), PLANE)
    returned = returned.astype(jnp.float32)
    summed = jnp.sum(returned[:, :rows].reshape(here, plane_size // here, rows, quarter), 1)
    summed = summed.reshape(here, planes, capacity, quarter).swapaxes(0, 1)
    dense_sum = jnp.sum(
        returned[:, rows:].reshape(plane_blocks, tp_size, dense_count, quarter), 0
    ).reshape(planes, part, quarter)
    back = jnp.concatenate([summed.reshape(planes, slots, quarter), dense_sum], 1)
    back = exchange(back.astype(jnp.bfloat16), "z").reshape(planes * (slots + part), quarter)
    branch = jax.nn.sigmoid(jnp.dot(x_mid, branch_gate, preferred_element_type=jnp.float32))
    factors = jnp.sum(jnp.where(slot_match, route_weights[:, :, None], 0.0), 1)
    factors = factors + jnp.where(row_match, branch[:, None], 0.0)
    second_sum = residual_scale * own_columns.astype(jnp.float32) + jnp.dot(
        factors,
        back.astype(jnp.float32),
        precision=lax.Precision.HIGHEST,
        preferred_element_type=jnp.float32,
    )
    row_sums, square_sums = in_one(
        (jnp.sum(second_sum, 1), jnp.sum(second_sum * second_sum, 1)), "tp"
    )
    average = row_sums / model_width
    spread = square_sums / model_width - average * average
    return (
        (second_sum - average[:, None]) * lax.rsqrt(spread + norm_epsilon)[:, None] * second_gain
    ).astype(jnp.bfloat16)


def solution(mesh):
    finer = Mesh(mesh.devices.reshape(16, 4, 2, mesh.shape["tp"]), ("z", "x", "c", "tp"))
    return jax.shard_map(
        shards,
        mesh=finer,
        in_specs=(
            P(EP, None),
            P(EP, "tp", None, None),
            P(None, "tp"),
            P(None, "tp"),
            P(None, "tp"),
            P("tp", None),
            P("tp"),
            P(),
            P(None, "tp"),
            P("tp"),
            P(),
            P(None, "tp"),
            P("tp"),
            P(),
            P(EP, None, "tp"),
            P(EP, None, "tp"),
            P(EP, "tp", None),
            P(EP, None),
            P(EP, None),
            P(EP, "tp"),
            P(),
            P("tp"),
            P(EP, None),
            P(EP, None),
        ),
        out_specs=P(EP, "tp"),
        check_vma=False,
    )
```

```python
import math

import jax
import jax.numpy as jnp
from jax import lax
from jax.experimental import pallas as pl
from jax.experimental.pallas import tpu as pltpu
from jax.sharding import Mesh
from jax.sharding import PartitionSpec as P


SPLIT = 4
EP = ("z", "x", "c")
PLANE = ("x", "c", "tp")


residual_scale = 1.4142135623730951
norm_epsilon = 1e-05
head_epsilon = 0.00064
key_epsilon = 1e-06


def sent_to_all(value, axis):
    copies = jnp.broadcast_to(value, (lax.axis_size(axis), *value.shape))
    return lax.all_to_all(copies, axis, split_axis=0, concat_axis=0, tiled=True)


def of_everyone(value, axis):
    return sent_to_all(value, axis).astype(jnp.float32).sum(axis=0)


def exchange(parts, axis):
    return lax.all_to_all(parts, axis, split_axis=0, concat_axis=0, tiled=True)


def in_one(arrays, axis):
    vector, at, done = (jnp.concatenate([a.reshape(-1) for a in arrays]), 0, [])
    running = of_everyone(vector, axis)
    for a in arrays:
        done.append(running[at : at + a.size].reshape(a.shape))
        at += a.size
    return tuple(done)


def padded_units(columns, multiple):
    return jnp.pad(columns, ((0, -columns.shape[0] % multiple), (0, 0)))


def with_neighbour(units, step):
    planes = lax.axis_size("z")
    other = lax.ppermute(units, "z", [(i, i ^ step) for i in range(planes)])
    return jnp.concatenate([units, other], 0)


def mixer_kernel(
    tokens_ref,
    down_ref,
    decay_base_ref,
    decay_up_ref,
    rate_base_ref,
    rate_up_ref,
    head_gain_ref,
    decay_down_any,
    rate_down_any,
    w_key_any,
    w_recep_any,
    w_value_any,
    state_any,
    w_out_any,
    message_ref,
    decay_down_ref,
    rate_down_ref,
    w_key_ref,
    w_recep_ref,
    w_value_ref,
    state_ref,
    w_out_ref,
    query_ref,
    answer_ref,
    arrival,
):
    copies = []
    for source, target in (
        (decay_down_any, decay_down_ref),
        (rate_down_any, rate_down_ref),
        (w_key_any, w_key_ref),
        (w_recep_any, w_recep_ref),
        (w_value_any, w_value_ref),
        (state_any, state_ref),
        (w_out_any, w_out_ref),
    ):
        copies.append(pltpu.make_async_copy(source, target, arrival.at[len(copies)]))
    for copy in copies:
        copy.start()
    row_count, heads, head_size = state_ref.shape[0], state_ref.shape[1], state_ref.shape[3]
    width = heads * head_size
    tokens = tokens_ref[...]
    f32 = jnp.float32

    def turned(a, b):
        return lax.dot_general(a, b, (((1,), (1,)), ((), ())), preferred_element_type=f32)

    channel_head = lax.broadcasted_iota(jnp.int32, (width, width), 0) // head_size
    same_head = (
        channel_head == lax.broadcasted_iota(jnp.int32, (width, width), 1) // head_size
    ).astype(f32)

    def over_head(values):
        return jnp.dot(
            values, same_head, precision=lax.Precision.HIGHEST, preferred_element_type=f32
        )

    copies[0].wait()
    decay_low = jnp.tanh(turned(tokens, decay_down_ref[...])).astype(jnp.bfloat16)
    copies[1].wait()
    rate_low = turned(tokens, rate_down_ref[...]).astype(jnp.bfloat16)
    decay_pre = decay_base_ref[...] + jnp.dot(
        decay_low, decay_up_ref[...], preferred_element_type=f32
    )
    decay = jnp.exp(-(math.exp(-0.5) * jax.nn.sigmoid(decay_pre)))
    in_rate = jax.nn.sigmoid(
        rate_base_ref[...] + jnp.dot(rate_low, rate_up_ref[...], preferred_element_type=f32)
    )
    copies[2].wait()
    key_vecs = jnp.dot(tokens, w_key_ref[...], preferred_element_type=f32)
    copies[3].wait()
    recep = jnp.dot(tokens, w_recep_ref[...], preferred_element_type=f32)
    sums = over_head(
        jnp.concatenate([key_vecs * key_vecs, key_vecs * in_rate * recep, key_vecs * recep], 0)
    )
    scale = lax.rsqrt(sums[:row_count] + key_epsilon)
    removed_factor = scale * sums[row_count : 2 * row_count]
    value_factor = sums[2 * row_count :]
    for which, vectors in enumerate((decay * recep, key_vecs * scale)):
        for h in range(heads):
            pair = vectors[:, h // 2 * 128 : h // 2 * 128 + 128]
            query_ref[pl.ds(which * heads + h, row_count, stride=2 * heads), :] = (
                pair if h % 2 == 0 else pltpu.roll(pair, head_size, 1)
            )
    copies[4].wait()
    value_vecs = jnp.dot(tokens, w_value_ref[...], preferred_element_type=f32)
    copies[5].wait()
    for t in range(row_count):
        queries = query_ref[2 * heads * t : 2 * heads * (t + 1), :head_size].astype(jnp.bfloat16)
        matrix = state_ref[t].reshape(width, head_size).astype(jnp.bfloat16)
        answers = turned(queries, matrix)
        for pair in range(heads // 2):
            answer_ref[pair, 2 * heads * t : 2 * heads * (t + 1), :] = answers[
                :, pair * 128 : (pair + 1) * 128
            ]
    first_of_pair = lax.broadcasted_iota(jnp.int32, (row_count, 128), 1) < head_size

    def picked(which):
        pairs = []
        for pair in range(heads // 2):
            of_pair = answer_ref.at[pair]
            rows = [
                of_pair[pl.ds(which * heads + 2 * pair + i, row_count, stride=2 * heads), :]
                for i in range(2)
            ]
            pairs.append(jnp.where(first_of_pair, rows[0], rows[1]))
        return jnp.concatenate(pairs, 1)

    read_out = picked(0) - picked(1) * removed_factor + value_vecs * value_factor
    centred = read_out - over_head(read_out) * (1.0 / head_size)
    spread = over_head(centred * centred) * (1.0 / head_size)
    normed = centred * lax.rsqrt(spread + head_epsilon) * head_gain_ref[...]
    copies[6].wait()
    mixed = jnp.dot(normed.astype(jnp.bfloat16), w_out_ref[...], preferred_element_type=f32)
    mixed = mixed.astype(jnp.bfloat16)
    copies_out, mix_rows = message_ref.shape[0], row_count * heads
    for c in range(copies_out):
        for h in range(mixed.shape[1] // width):
            message_ref[c, h * row_count : (h + 1) * row_count, :] = mixed[
                :, h * width : (h + 1) * width
            ]
        message_ref[c, mix_rows:, :] = jnp.zeros_like(message_ref[c, mix_rows:, :])
        message_ref[c, mix_rows : mix_rows + down_ref.shape[0], :] = down_ref[...]


def mixer_message(
    copies_out,
    own_down,
    tokens,
    state,
    w_recep,
    w_key,
    w_value,
    w_out,
    decay_base,
    decay_down,
    decay_up,
    rate_base,
    rate_down,
    rate_up,
    head_gain,
):
    row_count, heads, head_size = state.shape[0], state.shape[1], state.shape[3]
    width = heads * head_size
    here = [
        tokens,
        own_down,
        decay_base[None],
        decay_up,
        rate_base[None],
        rate_up,
        head_gain[None],
    ]
    far = [decay_down.T, rate_down.T, w_key, w_recep, w_value, state, w_out]
    down_rows = own_down.shape[0] + -own_down.shape[0] % 8
    rows = tokens.shape[1] // width * row_count + down_rows
    return pl.pallas_call(
        mixer_kernel,
        out_shape=jax.ShapeDtypeStruct((copies_out, rows, width), jnp.bfloat16),
        in_specs=[pl.BlockSpec(memory_space=pltpu.VMEM)] * len(here)
        + [pl.BlockSpec(memory_space=pl.ANY)] * len(far),
        out_specs=pl.BlockSpec(memory_space=pltpu.VMEM),
        scratch_shapes=[pltpu.VMEM(a.shape, a.dtype) for a in far]
        + [
            pltpu.VMEM((2 * heads * row_count, 128), jnp.float32),
            pltpu.VMEM((heads // 2, 2 * heads * row_count, 128), jnp.float32),
            pltpu.SemaphoreType.DMA((len(far),)),
        ],
        name="mixer",
    )(*here, *far)


def first_norm(values, gain):
    centre = jnp.mean(values, -1, keepdims=True)
    spread = jnp.mean(jnp.square(values - centre), -1, keepdims=True)
    return ((values - centre) * lax.rsqrt(spread + norm_epsilon) * gain).astype(jnp.bfloat16)


def route_targets(routes, experts, capacity):
    expert_hits = (
        routes[:, :, None] == jnp.arange(experts, dtype=jnp.int32)[None, None, :]
    ).astype(jnp.int32)
    row_hits = jnp.sum(expert_hits, 1, dtype=jnp.int32)
    earlier = jnp.cumsum(row_hits, 0, dtype=jnp.int32) - row_hits
    slot_index = jnp.sum(earlier[:, None, :] * expert_hits, 2, dtype=jnp.int32)
    return routes * capacity + slot_index


def shards(
    tokens,
    state,
    w_recep,
    w_key,
    w_value,
    w_out,
    decay_base,
    decay_down,
    decay_up,
    rate_base,
    rate_down,
    rate_up,
    head_gain,
    first_gain,
    expert_gate,
    expert_up,
    expert_down,
    dense_gate,
    dense_up,
    dense_down,
    branch_gate,
    second_gain,
    routes,
    route_weights,
):
    row_count = tokens.shape[0]
    model_width = tokens.shape[1]
    quarter = w_recep.shape[1]
    tp_index = lax.axis_index("tp")
    planes = lax.axis_size("z")
    plane_blocks = lax.axis_size(("x", "c"))
    plane_size = lax.axis_size(PLANE)
    tp_size = lax.axis_size("tp")
    shared = planes // tp_size
    message = mixer_message(
        tp_size,
        dense_down,
        tokens,
        state,
        w_recep,
        w_key,
        w_value,
        w_out,
        decay_base,
        decay_down,
        decay_up,
        rate_base,
        rate_down,
        rate_up,
        head_gain,
    )
    everyone = exchange(message, "tp")
    mix_rows = tp_size * row_count
    mixed = jnp.sum(everyone[:, :mix_rows].astype(jnp.float32), 0)
    mixed = jnp.concatenate(
        [mixed[i * row_count : (i + 1) * row_count] for i in range(tp_size)], 1
    )
    units = jnp.concatenate(
        [padded_units(dense_gate, 8), padded_units(dense_up, 8)]
        + [everyone[i, mix_rows:] for i in range(tp_size)],
        1,
    )
    units = with_neighbour(units, 2)
    units = with_neighbour(units, 1)
    x_mid = first_norm(residual_scale * tokens.astype(jnp.float32) + mixed, first_gain)
    own_columns = lax.dynamic_slice_in_dim(x_mid, tp_index * quarter, quarter, 1)
    experts = lax.axis_size(EP) // SPLIT
    here = experts // planes
    capacity = min(row_count, max(2, 2 * row_count * routes.shape[1] // experts))
    slots = here * capacity
    part = row_count // shared
    target = route_targets(routes, experts, capacity)
    place = jnp.arange(planes * (slots + part), dtype=jnp.int32)
    plane, inner = place // (slots + part), place % (slots + part)
    routed_place = jnp.where(inner < slots, plane * slots + inner, -1)
    dense_place = jnp.where(inner < slots, -1, plane % shared * part + inner - slots)
    slot_match = target[:, :, None] == routed_place[None, None, :]
    row_match = jnp.arange(row_count, dtype=jnp.int32)[:, None] == dense_place[None, :]
    chosen = (jnp.any(slot_match, 1) | row_match).astype(jnp.bfloat16)
    packed_rows = lax.dot_general(
        chosen, own_columns, (((0,), (0,)), ((), ())), preferred_element_type=jnp.float32
    ).astype(jnp.bfloat16)
    arrived = exchange(packed_rows.reshape(planes, slots + part, quarter), "z")
    rows = planes * capacity
    dense_count = shared * part
    height = rows + dense_count
    routed_rows = arrived[:, :slots].reshape(planes, here, capacity, quarter).swapaxes(0, 1)
    routed_rows = routed_rows.reshape(here, 1, 1, rows, quarter)
    dense_rows = arrived[:, slots:].reshape(1, 1, tp_size, dense_count, quarter)
    wide = (here, plane_blocks // here, tp_size)
    outgoing = jnp.concatenate(
        [
            jnp.broadcast_to(routed_rows, (*wide, rows, quarter)),
            jnp.broadcast_to(dense_rows, (*wide, dense_count, quarter)),
        ],
        3,
    )
    everything = exchange(outgoing.reshape(plane_size, height, quarter), PLANE)
    everything = everything.reshape(plane_blocks, tp_size, height, quarter).swapaxes(1, 2)
    everything = everything.reshape(plane_blocks, height, model_width)
    flat_rows = everything[:, :rows].reshape(plane_blocks * rows, model_width)
    dense_rows = everything[:, rows:].reshape(plane_blocks * dense_count, model_width)
    gate_pre = jnp.dot(flat_rows, expert_gate[0], preferred_element_type=jnp.float32)
    up_pre = jnp.dot(flat_rows, expert_up[0], preferred_element_type=jnp.float32)
    hidden = (jax.nn.silu(gate_pre) * up_pre).astype(jnp.bfloat16)
    partial_out = jnp.dot(hidden, expert_down[0], preferred_element_type=jnp.float32)
    dense_pre = [
        lax.dot_general(
            dense_rows,
            units[:, i * model_width : (i + 1) * model_width],
            (((1,), (1,)), ((), ())),
            preferred_element_type=jnp.float32,
        )
        for i in range(2)
    ]
    dense_hidden = (jax.nn.silu(dense_pre[0]) * dense_pre[1]).astype(jnp.bfloat16)
    partial_out = partial_out.astype(jnp.bfloat16)
    returning = jnp.stack(
        [
            jnp.concatenate(
                [
                    partial_out[:, i * quarter : (i + 1) * quarter].reshape(
                        plane_blocks, rows, quarter
                    ),
                    jnp.dot(
                        dense_hidden,
                        units[:, 2 * model_width + i * quarter :][:, :quarter],
                        preferred_element_type=jnp.float32,
                    )
                    .astype(jnp.bfloat16)
                    .reshape(plane_blocks, dense_count, quarter),
                ],
                1,
            )
            for i in range(tp_size)
        ],
        1,
    )
    returned = exchange(returning.reshape(plane_size, height, quarter), PLANE)
    returned = returned.astype(jnp.float32)
    summed = jnp.sum(returned[:, :rows].reshape(here, plane_size // here, rows, quarter), 1)
    summed = summed.reshape(here, planes, capacity, quarter).swapaxes(0, 1)
    dense_sum = jnp.sum(
        returned[:, rows:].reshape(plane_blocks, tp_size, dense_count, quarter), 0
    ).reshape(planes, part, quarter)
    back = jnp.concatenate([summed.reshape(planes, slots, quarter), dense_sum], 1)
    back = exchange(back.astype(jnp.bfloat16), "z").reshape(planes * (slots + part), quarter)
    branch = jax.nn.sigmoid(jnp.dot(x_mid, branch_gate, preferred_element_type=jnp.float32))
    factors = jnp.sum(jnp.where(slot_match, route_weights[:, :, None], 0.0), 1)
    factors = factors + jnp.where(row_match, branch[:, None], 0.0)
    second_sum = residual_scale * own_columns.astype(jnp.float32) + jnp.dot(
        factors,
        back.astype(jnp.float32),
        precision=lax.Precision.HIGHEST,
        preferred_element_type=jnp.float32,
    )
    row_sums, square_sums = in_one(
        (jnp.sum(second_sum, 1), jnp.sum(second_sum * second_sum, 1)), "tp"
    )
    average = row_sums / model_width
    spread = square_sums / model_width - average * average
    return (
        (second_sum - average[:, None]) * lax.rsqrt(spread + norm_epsilon)[:, None] * second_gain
    ).astype(jnp.bfloat16)


def solution(mesh):
    finer = Mesh(mesh.devices.reshape(16, 4, 2, mesh.shape["tp"]), ("z", "x", "c", "tp"))
    return jax.shard_map(
        shards,
        mesh=finer,
        in_specs=(
            P(EP, None),
            P(EP, "tp", None, None),
            P(None, "tp"),
            P(None, "tp"),
            P(None, "tp"),
            P("tp", None),
            P("tp"),
            P(),
            P(None, "tp"),
            P("tp"),
            P(),
            P(None, "tp"),
            P("tp"),
            P(),
            P(EP, None, "tp"),
            P(EP, None, "tp"),
            P(EP, "tp", None),
            P(EP, None),
            P(EP, None),
            P(EP, "tp"),
            P(),
            P("tp"),
            P(EP, None),
            P(EP, None),
        ),
        out_specs=P(EP, "tp"),
        check_vma=False,
    )
```

```python
import math
from functools import partial

import jax
import jax.numpy as jnp
from jax import lax
from jax.experimental import pallas as pl
from jax.experimental.pallas import tpu as pltpu
from jax.sharding import Mesh
from jax.sharding import PartitionSpec as P


SPLIT = 4
EP = ("z", "x", "c")
PLANE = ("x", "c", "tp")


residual_scale = 1.4142135623730951
norm_epsilon = 1e-05
head_epsilon = 0.00064
key_epsilon = 1e-06


def sent_to_all(value, axis):
    copies = jnp.broadcast_to(value, (lax.axis_size(axis), *value.shape))
    return lax.all_to_all(copies, axis, split_axis=0, concat_axis=0, tiled=True)


def of_everyone(value, axis):
    return sent_to_all(value, axis).astype(jnp.float32).sum(axis=0)


def exchange(parts, axis):
    return lax.all_to_all(parts, axis, split_axis=0, concat_axis=0, tiled=True)


def in_one(arrays, axis):
    vector, at, done = (jnp.concatenate([a.reshape(-1) for a in arrays]), 0, [])
    running = of_everyone(vector, axis)
    for a in arrays:
        done.append(running[at : at + a.size].reshape(a.shape))
        at += a.size
    return tuple(done)


def padded_units(columns, multiple):
    return jnp.pad(columns, ((0, -columns.shape[0] % multiple), (0, 0)))


def with_neighbour(units, step):
    planes = lax.axis_size("z")
    other = lax.ppermute(units, "z", [(i, i ^ step) for i in range(planes)])
    return jnp.concatenate([units, other], 0)


def mixer_kernel(*refs, chunks):
    count = (len(refs) - 4) // 2
    sources, message_ref, targets = refs[:count], refs[count], refs[count + 1 : 2 * count + 1]
    query_ref, answer_ref, arrival = refs[2 * count + 1 :]
    (
        tokens_ref,
        decay_down_ref,
        rate_down_ref,
        decay_up_ref,
        decay_base_ref,
        rate_up_ref,
        rate_base_ref,
        w_key_ref,
        w_recep_ref,
        state_ref,
        w_value_ref,
        head_gain_ref,
        w_out_ref,
        down_ref,
    ) = targets
    copies = {}
    for source, target in zip(sources, targets):
        parts = chunks if target is state_ref else 1
        size = target.shape[0] // parts
        for i in range(parts):
            at = pl.ds(i * size, size) if parts > 1 else slice(None)
            copies[id(target), i] = pltpu.make_async_copy(
                source.at[at], target.at[at], arrival.at[len(copies)]
            )
    for copy in copies.values():
        copy.start()

    def landed(target, part=0):
        copies[id(target), part].wait()
        return target

    row_count, heads, head_size = state_ref.shape[0], state_ref.shape[1], state_ref.shape[3]
    width = heads * head_size
    tokens = landed(tokens_ref)[...]
    f32 = jnp.float32

    def turned(a, b):
        return lax.dot_general(a, b, (((1,), (1,)), ((), ())), preferred_element_type=f32)

    channel_head = lax.broadcasted_iota(jnp.int32, (width, width), 0) // head_size
    same_head = (
        channel_head == lax.broadcasted_iota(jnp.int32, (width, width), 1) // head_size
    ).astype(f32)

    def over_head(values):
        return jnp.dot(
            values, same_head, precision=lax.Precision.HIGHEST, preferred_element_type=f32
        )

    decay_low = jnp.tanh(turned(tokens, landed(decay_down_ref)[...])).astype(jnp.bfloat16)
    rate_low = turned(tokens, landed(rate_down_ref)[...]).astype(jnp.bfloat16)
    decay_pre = landed(decay_base_ref)[...] + jnp.dot(
        decay_low, landed(decay_up_ref)[...], preferred_element_type=f32
    )
    decay = jnp.exp(-(math.exp(-0.5) * jax.nn.sigmoid(decay_pre)))
    in_rate = jax.nn.sigmoid(
        landed(rate_base_ref)[...]
        + jnp.dot(rate_low, landed(rate_up_ref)[...], preferred_element_type=f32)
    )
    key_vecs = jnp.dot(tokens, landed(w_key_ref)[...], preferred_element_type=f32)
    recep = jnp.dot(tokens, landed(w_recep_ref)[...], preferred_element_type=f32)
    sums = over_head(
        jnp.concatenate([key_vecs * key_vecs, key_vecs * in_rate * recep, key_vecs * recep], 0)
    )
    scale = lax.rsqrt(sums[:row_count] + key_epsilon)
    removed_factor = scale * sums[row_count : 2 * row_count]
    value_factor = sums[2 * row_count :]
    for which, vectors in enumerate((decay * recep, key_vecs * scale)):
        for h in range(heads):
            pair = vectors[:, h // 2 * 128 : h // 2 * 128 + 128]
            query_ref[pl.ds(which * heads + h, row_count, stride=2 * heads), :] = (
                pair if h % 2 == 0 else pltpu.roll(pair, head_size, 1)
            )
    for t in range(row_count):
        if t % (row_count // chunks) == 0:
            landed(state_ref, t // (row_count // chunks))
        queries = query_ref[2 * heads * t : 2 * heads * (t + 1), :head_size].astype(jnp.bfloat16)
        matrix = state_ref[t].reshape(width, head_size).astype(jnp.bfloat16)
        answers = turned(queries, matrix)
        for pair in range(heads // 2):
            answer_ref[pair, 2 * heads * t : 2 * heads * (t + 1), :] = answers[
                :, pair * 128 : (pair + 1) * 128
            ]
    first_of_pair = lax.broadcasted_iota(jnp.int32, (row_count, 128), 1) < head_size

    def picked(which):
        pairs = []
        for pair in range(heads // 2):
            of_pair = answer_ref.at[pair]
            rows = [
                of_pair[pl.ds(which * heads + 2 * pair + i, row_count, stride=2 * heads), :]
                for i in range(2)
            ]
            pairs.append(jnp.where(first_of_pair, rows[0], rows[1]))
        return jnp.concatenate(pairs, 1)

    value_vecs = jnp.dot(tokens, landed(w_value_ref)[...], preferred_element_type=f32)
    read_out = picked(0) - picked(1) * removed_factor + value_vecs * value_factor
    centred = read_out - over_head(read_out) * (1.0 / head_size)
    spread = over_head(centred * centred) * (1.0 / head_size)
    normed = centred * lax.rsqrt(spread + head_epsilon) * landed(head_gain_ref)[...]
    mixed = jnp.dot(normed.astype(jnp.bfloat16), landed(w_out_ref)[...], preferred_element_type=f32)
    mixed = mixed.astype(jnp.bfloat16)
    copies_out, mix_rows = message_ref.shape[0], row_count * heads
    landed(down_ref)
    for c in range(copies_out):
        for h in range(mixed.shape[1] // width):
            message_ref[c, h * row_count : (h + 1) * row_count, :] = mixed[
                :, h * width : (h + 1) * width
            ]
        message_ref[c, mix_rows:, :] = jnp.zeros_like(message_ref[c, mix_rows:, :])
        message_ref[c, mix_rows : mix_rows + down_ref.shape[0], :] = down_ref[...]


def mixer_message(
    copies_out,
    own_down,
    tokens,
    state,
    w_recep,
    w_key,
    w_value,
    w_out,
    decay_base,
    decay_down,
    decay_up,
    rate_base,
    rate_down,
    rate_up,
    head_gain,
):
    row_count, heads, head_size = state.shape[0], state.shape[1], state.shape[3]
    width = heads * head_size
    far = [
        tokens,
        decay_down.T,
        rate_down.T,
        decay_up,
        decay_base[None],
        rate_up,
        rate_base[None],
        w_key,
        w_recep,
        state,
        w_value,
        head_gain[None],
        w_out,
        own_down,
    ]
    chunks = 4
    down_rows = own_down.shape[0] + -own_down.shape[0] % 8
    rows = tokens.shape[1] // width * row_count + down_rows
    return pl.pallas_call(
        partial(mixer_kernel, chunks=chunks),
        out_shape=pltpu.VMEM((copies_out, rows, width), jnp.bfloat16),
        in_specs=[pl.BlockSpec(memory_space=pl.ANY)] * len(far),
        out_specs=pl.BlockSpec(memory_space=pltpu.VMEM),
        scratch_shapes=[pltpu.VMEM(a.shape, a.dtype) for a in far]
        + [
            pltpu.VMEM((2 * heads * row_count, 128), jnp.float32),
            pltpu.VMEM((heads // 2, 2 * heads * row_count, 128), jnp.float32),
            pltpu.SemaphoreType.DMA((len(far) - 1 + chunks,)),
        ],
        name="mixer",
    )(*far)


def expert_kernel(
    rows_ref,
    units_ref,
    gate_any,
    up_any,
    down_any,
    out_ref,
    gate_ref,
    up_ref,
    down_ref,
    arrival,
    *,
    rows,
):
    copies = [
        pltpu.make_async_copy(source, target, arrival.at[i])
        for i, (source, target) in enumerate(
            ((gate_any, gate_ref), (up_any, up_ref), (down_any, down_ref))
        )
    ]
    for copy in copies:
        copy.start()
    blocks, splits, height, quarter = rows_ref.shape
    width = splits * quarter
    f32 = jnp.float32

    def turned(a, b):
        return lax.dot_general(a, b, (((1,), (1,)), ((), ())), preferred_element_type=f32)

    def whole_rows(low, high):
        return jnp.concatenate(
            [
                rows_ref[:, i, low:high, :].reshape(blocks * (high - low), quarter)
                for i in range(splits)
            ],
            1,
        )

    dense = whole_rows(rows, height)
    gate_pre = turned(dense, units_ref[:, :width])
    up_pre = turned(dense, units_ref[:, width : 2 * width])
    hidden = (jax.nn.silu(gate_pre) * up_pre).astype(jnp.bfloat16)
    for i in range(splits):
        down = units_ref[:, 2 * width + i * quarter : 2 * width + (i + 1) * quarter]
        part = jnp.dot(hidden, down, preferred_element_type=f32).astype(jnp.bfloat16)
        out_ref[:, i, rows:, :] = part.reshape(blocks, height - rows, quarter)
    routed = whole_rows(0, rows)
    copies[0].wait()
    gate_pre = turned(routed, gate_ref[...])
    copies[1].wait()
    up_pre = turned(routed, up_ref[...])
    hidden = (jax.nn.silu(gate_pre) * up_pre).astype(jnp.bfloat16)
    copies[2].wait()
    for i in range(splits):
        down = down_ref[:, i * quarter : (i + 1) * quarter]
        part = jnp.dot(hidden, down, preferred_element_type=f32).astype(jnp.bfloat16)
        out_ref[:, i, :rows, :] = part.reshape(blocks, rows, quarter)


def run_experts(everything, units, expert_gate, expert_up, expert_down, rows):
    far = [expert_gate.T, expert_up.T, expert_down]
    vmem = pl.BlockSpec(memory_space=pltpu.VMEM)
    return pl.pallas_call(
        partial(expert_kernel, rows=rows),
        out_shape=pltpu.VMEM(everything.shape, jnp.bfloat16),
        in_specs=[vmem, vmem] + [pl.BlockSpec(memory_space=pl.ANY)] * len(far),
        out_specs=vmem,
        scratch_shapes=[pltpu.VMEM(a.shape, a.dtype) for a in far]
        + [pltpu.SemaphoreType.DMA((len(far),))],
        name="experts",
    )(on_chip(everything), on_chip(units), *far)


def on_chip(value):
    return pltpu.with_memory_space_constraint(value, pltpu.VMEM)


def norm_kernel(
    everyone_ref,
    tokens_ref,
    gain_ref,
    branch_gate_ref,
    routes_ref,
    route_weights_ref,
    packed_ref,
    own_ref,
    factors_ref,
    *,
    experts,
    capacity,
    slots,
    shared,
):
    splits, _, quarter = everyone_ref.shape
    row_count = tokens_ref.shape[0]
    f32, i32 = jnp.float32, jnp.int32
    mixed = everyone_ref[0, : splits * row_count, :].astype(f32)
    for s in range(1, splits):
        mixed = mixed + everyone_ref[s, : splits * row_count, :].astype(f32)
    mixed = jnp.concatenate(
        [mixed[i * row_count : (i + 1) * row_count] for i in range(splits)], 1
    )
    x_mid = first_norm(residual_scale * tokens_ref[...].astype(f32) + mixed, gain_ref[...])
    own = jnp.zeros((row_count, quarter), f32)
    for i in range(splits):
        columns = x_mid[:, i * quarter : (i + 1) * quarter].astype(f32)
        own = jnp.where(lax.axis_index("tp") == i, columns, own)
    own_ref[...] = own
    branch = jax.nn.sigmoid(
        lax.dot_general(
            branch_gate_ref[...], x_mid, (((1,), (1,)), ((), ())), preferred_element_type=f32
        )
    )
    first, second = routes_ref[0:1, :], routes_ref[1:2, :]
    expert = lax.broadcasted_iota(i32, (experts, row_count), 0)
    hit_first, hit_second = (expert == first).astype(f32), (expert == second).astype(f32)
    before = (
        lax.broadcasted_iota(i32, (row_count, row_count), 0)
        < lax.broadcasted_iota(i32, (row_count, row_count), 1)
    ).astype(f32)
    earlier = jnp.dot(hit_first + hit_second, before, preferred_element_type=f32)
    slot_first = jnp.sum(earlier * hit_first, 0, keepdims=True).astype(i32)
    slot_second = jnp.sum(earlier * hit_second, 0, keepdims=True).astype(i32)
    lines = packed_ref.shape[0]
    height = lines * slots // (experts * capacity)
    place = lax.broadcasted_iota(i32, (lines, row_count), 0)
    row = lax.broadcasted_iota(i32, (lines, row_count), 1)
    plane, inner = place // height, place % height
    routed_place = jnp.where(inner < slots, plane * slots + inner, -1)
    dense_place = jnp.where(
        inner < slots, -1, plane % shared * (height - slots) + inner - slots
    )
    at_first = routed_place == first * capacity + slot_first
    at_second = routed_place == second * capacity + slot_second
    at_row = dense_place == row
    chosen = (at_first | at_second | at_row).astype(jnp.bfloat16)
    packed_ref[...] = jnp.dot(
        chosen, own.astype(jnp.bfloat16), preferred_element_type=f32
    ).astype(jnp.bfloat16)
    factors = (
        jnp.where(at_first, route_weights_ref[0:1, :], 0.0)
        + jnp.where(at_second, route_weights_ref[1:2, :], 0.0)
        + jnp.where(at_row, branch, 0.0)
    )
    factors_ref[...] = factors


def norm_and_pack(
    everyone,
    tokens,
    first_gain,
    branch_gate,
    routes,
    route_weights,
    lines,
    experts,
    capacity,
    slots,
    shared,
):
    row_count, quarter = tokens.shape[0], everyone.shape[2]
    vmem = pl.BlockSpec(memory_space=pltpu.VMEM)
    return pl.pallas_call(
        partial(norm_kernel, experts=experts, capacity=capacity, slots=slots, shared=shared),
        out_shape=(
            pltpu.VMEM((lines, quarter), jnp.bfloat16),
            pltpu.VMEM((row_count, quarter), jnp.float32),
            pltpu.VMEM((lines, row_count), jnp.float32),
        ),
        in_specs=[vmem] * 6,
        out_specs=(vmem, vmem, vmem),
        name="norm_and_pack",
    )(
        on_chip(everyone),
        on_chip(tokens),
        on_chip(first_gain[None]),
        on_chip(branch_gate[None]),
        on_chip(routes.T),
        on_chip(route_weights.T),
    )


def fan_kernel(arrived_ref, out_ref, *, capacity, shared):
    planes, slots_part, quarter = arrived_ref.shape
    here, copies, splits, height, _ = out_ref.shape
    part = slots_part - here * capacity
    rows = planes * capacity
    shape = (here * splits * height, planes * slots_part)
    line = lax.broadcasted_iota(jnp.int32, shape, 0)
    column = lax.broadcasted_iota(jnp.int32, shape, 1)
    index, group = line % height, line // height
    expert, split = group // splits, group % splits
    dense = index - rows
    routed_from = index // capacity * slots_part + expert * capacity + index % capacity
    dense_from = (
        (split * shared + dense // part) * slots_part + here * capacity + dense % part
    )
    chosen = (column == jnp.where(index < rows, routed_from, dense_from)).astype(jnp.bfloat16)
    arrived = arrived_ref[...].reshape(planes * slots_part, quarter)
    laid = jnp.dot(chosen, arrived, preferred_element_type=jnp.float32).astype(jnp.bfloat16)
    for e in range(here):
        for i in range(splits):
            at = (e * splits + i) * height
            for c in range(copies):
                out_ref[e, c, i, :, :] = laid[at : at + height]


def fan_out(arrived, capacity, here, copies, splits, shared):
    planes, slots_part, quarter = arrived.shape
    height = planes * capacity + shared * (slots_part - here * capacity)
    vmem = pl.BlockSpec(memory_space=pltpu.VMEM)
    return pl.pallas_call(
        partial(fan_kernel, capacity=capacity, shared=shared),
        out_shape=pltpu.VMEM((here, copies, splits, height, quarter), jnp.bfloat16),
        in_specs=[vmem],
        out_specs=vmem,
        name="fan_out",
    )(on_chip(arrived))


def gather_kernel(returned_ref, out_ref, *, capacity, here, splits, shared):
    planes, slots_part, quarter = out_ref.shape
    sources, height, _ = returned_ref.shape
    part = slots_part - here * capacity
    rows = planes * capacity
    f32 = jnp.float32
    routed = []
    for e in range(here):
        total = jnp.zeros((rows, quarter), f32)
        for s in range(e * (sources // here), (e + 1) * (sources // here)):
            total = total + returned_ref[s, :rows, :].astype(f32)
        routed.append(total)
    dense = []
    for i in range(splits):
        total = jnp.zeros((height - rows, quarter), f32)
        for s in range(i, sources, splits):
            total = total + returned_ref[s, rows:, :].astype(f32)
        dense.append(total)
    sums = jnp.concatenate(routed + dense, 0).astype(jnp.bfloat16)
    shape = (planes * slots_part, sums.shape[0])
    line = lax.broadcasted_iota(jnp.int32, shape, 0)
    column = lax.broadcasted_iota(jnp.int32, shape, 1)
    z, inner = line // slots_part, line % slots_part
    routed_from = inner // capacity * rows + z * capacity + inner % capacity
    dense_from = here * rows + z * part + inner - here * capacity
    chosen = (
        column == jnp.where(inner < here * capacity, routed_from, dense_from)
    ).astype(jnp.bfloat16)
    laid = jnp.dot(chosen, sums, preferred_element_type=f32).astype(jnp.bfloat16)
    out_ref[...] = laid.reshape(planes, slots_part, quarter)


def gather_back(returned, planes, slots_part, capacity, here, splits, shared):
    vmem = pl.BlockSpec(memory_space=pltpu.VMEM)
    return pl.pallas_call(
        partial(gather_kernel, capacity=capacity, here=here, splits=splits, shared=shared),
        out_shape=pltpu.VMEM((planes, slots_part, returned.shape[2]), jnp.bfloat16),
        in_specs=[vmem],
        out_specs=vmem,
        name="gather_back",
    )(on_chip(returned))


def first_norm(values, gain):
    centre = jnp.mean(values, -1, keepdims=True)
    spread = jnp.mean(jnp.square(values - centre), -1, keepdims=True)
    return ((values - centre) * lax.rsqrt(spread + norm_epsilon) * gain).astype(jnp.bfloat16)


def shards(
    tokens,
    state,
    w_recep,
    w_key,
    w_value,
    w_out,
    decay_base,
    decay_down,
    decay_up,
    rate_base,
    rate_down,
    rate_up,
    head_gain,
    first_gain,
    expert_gate,
    expert_up,
    expert_down,
    dense_gate,
    dense_up,
    dense_down,
    branch_gate,
    second_gain,
    routes,
    route_weights,
):
    row_count = tokens.shape[0]
    model_width = tokens.shape[1]
    quarter = w_recep.shape[1]
    planes = lax.axis_size("z")
    plane_blocks = lax.axis_size(("x", "c"))
    plane_size = lax.axis_size(PLANE)
    tp_size = lax.axis_size("tp")
    shared = planes // tp_size
    message = mixer_message(
        tp_size,
        dense_down,
        tokens,
        state,
        w_recep,
        w_key,
        w_value,
        w_out,
        decay_base,
        decay_down,
        decay_up,
        rate_base,
        rate_down,
        rate_up,
        head_gain,
    )
    everyone = exchange(message, "tp")
    everyone, dense_gate, dense_up, branch_gate = lax.optimization_barrier(
        (everyone, dense_gate, dense_up, branch_gate)
    )
    mix_rows = tp_size * row_count
    units = jnp.concatenate(
        [padded_units(dense_gate, 8), padded_units(dense_up, 8)]
        + [everyone[i, mix_rows:] for i in range(tp_size)],
        1,
    )
    units = with_neighbour(units, 2)
    units = with_neighbour(units, 1)
    experts = lax.axis_size(EP) // SPLIT
    here = experts // planes
    capacity = min(row_count, max(2, 2 * row_count * routes.shape[1] // experts))
    slots = here * capacity
    part = row_count // shared
    packed_rows, own_columns, factors = norm_and_pack(
        everyone,
        tokens,
        first_gain,
        branch_gate,
        routes,
        route_weights,
        planes * (slots + part),
        experts,
        capacity,
        slots,
        shared,
    )
    arrived = exchange(packed_rows.reshape(planes, slots + part, quarter), "z")
    rows = planes * capacity
    dense_count = shared * part
    height = rows + dense_count
    outgoing = fan_out(arrived, capacity, here, plane_blocks // here, tp_size, shared)
    everything = exchange(outgoing.reshape(plane_size, height, quarter), PLANE)
    everything = everything.reshape(plane_blocks, tp_size, height, quarter)
    returning = run_experts(
        everything, units, expert_gate[0], expert_up[0], expert_down[0], rows
    )
    returned = exchange(returning.reshape(plane_size, height, quarter), PLANE)
    back = gather_back(returned, planes, slots + part, capacity, here, tp_size, shared)
    back = exchange(back, "z").reshape(planes * (slots + part), quarter)
    second_sum = residual_scale * own_columns + lax.dot_general(
        factors,
        back.astype(jnp.float32),
        (((0,), (0,)), ((), ())),
        precision=lax.Precision.HIGHEST,
        preferred_element_type=jnp.float32,
    )
    row_sums, square_sums = in_one(
        (jnp.sum(second_sum, 1), jnp.sum(second_sum * second_sum, 1)), "tp"
    )
    average = row_sums / model_width
    spread = square_sums / model_width - average * average
    return (
        (second_sum - average[:, None]) * lax.rsqrt(spread + norm_epsilon)[:, None] * second_gain
    ).astype(jnp.bfloat16)


def solution(mesh):
    finer = Mesh(mesh.devices.reshape(16, 4, 2, mesh.shape["tp"]), ("z", "x", "c", "tp"))
    return jax.shard_map(
        shards,
        mesh=finer,
        in_specs=(
            P(EP, None),
            P(EP, "tp", None, None),
            P(None, "tp"),
            P(None, "tp"),
            P(None, "tp"),
            P("tp", None),
            P("tp"),
            P(),
            P(None, "tp"),
            P("tp"),
            P(),
            P(None, "tp"),
            P("tp"),
            P(),
            P(EP, None, "tp"),
            P(EP, None, "tp"),
            P(EP, "tp", None),
            P(EP, None),
            P(EP, None),
            P(EP, "tp"),
            P(),
            P("tp"),
            P(EP, None),
            P(EP, None),
        ),
        out_specs=P(EP, "tp"),
        check_vma=False,
    )
```

```python
import math
from functools import partial

import jax
import jax.numpy as jnp
import numpy as np
from jax import lax
from jax.experimental import pallas as pl
from jax.experimental.pallas import tpu as pltpu
from jax.sharding import Mesh
from jax.sharding import PartitionSpec as P


SPLIT = 4
EP = ("z", "x", "c")
PLANE = ("x", "c", "tp")


residual_scale = 1.4142135623730951
norm_epsilon = 1e-05
head_epsilon = 0.00064
key_epsilon = 1e-06


def sent_to_all(value, axis):
    copies = jnp.broadcast_to(value, (lax.axis_size(axis), *value.shape))
    return lax.all_to_all(copies, axis, split_axis=0, concat_axis=0, tiled=True)


def of_everyone(value, axis):
    return sent_to_all(value, axis).astype(jnp.float32).sum(axis=0)


def exchange(parts, axis):
    return lax.all_to_all(parts, axis, split_axis=0, concat_axis=0, tiled=True)


def in_one(arrays, axis):
    vector, at, done = (jnp.concatenate([a.reshape(-1) for a in arrays]), 0, [])
    running = of_everyone(vector, axis)
    for a in arrays:
        done.append(running[at : at + a.size].reshape(a.shape))
        at += a.size
    return tuple(done)


def padded_units(columns, multiple):
    return jnp.pad(columns, ((0, -columns.shape[0] % multiple), (0, 0)))


def with_neighbour(units, step):
    planes = lax.axis_size("z")
    other = lax.ppermute(units, "z", [(i, i ^ step) for i in range(planes)])
    return jnp.concatenate([units, other], 0)


def mixer_kernel(*refs, chunks):
    count = (len(refs) - 4) // 2
    sources, message_ref, targets = refs[:count], refs[count], refs[count + 1 : 2 * count + 1]
    query_ref, answer_ref, arrival = refs[2 * count + 1 :]
    (
        tokens_ref,
        decay_down_ref,
        rate_down_ref,
        decay_up_ref,
        decay_base_ref,
        rate_up_ref,
        rate_base_ref,
        w_key_ref,
        w_recep_ref,
        state_ref,
        w_value_ref,
        head_gain_ref,
        w_out_ref,
        down_ref,
    ) = targets
    copies = {}
    for source, target in zip(sources, targets):
        parts = chunks if target is state_ref else 1
        size = target.shape[0] // parts
        for i in range(parts):
            at = pl.ds(i * size, size) if parts > 1 else slice(None)
            copies[id(target), i] = pltpu.make_async_copy(
                source.at[at], target.at[at], arrival.at[len(copies)]
            )
    for copy in copies.values():
        copy.start()

    def landed(target, part=0):
        copies[id(target), part].wait()
        return target

    row_count, heads, head_size = state_ref.shape[0], state_ref.shape[1], state_ref.shape[3]
    width = heads * head_size
    tokens = landed(tokens_ref)[...]
    f32 = jnp.float32

    def turned(a, b):
        return lax.dot_general(a, b, (((1,), (1,)), ((), ())), preferred_element_type=f32)

    channel_head = lax.broadcasted_iota(jnp.int32, (width, width), 0) // head_size
    same_head = (
        channel_head == lax.broadcasted_iota(jnp.int32, (width, width), 1) // head_size
    ).astype(jnp.bfloat16)

    def over_head(values):
        high = values.astype(jnp.bfloat16)
        rest = values - high.astype(f32)
        middle = rest.astype(jnp.bfloat16)
        low = (rest - middle.astype(f32)).astype(jnp.bfloat16)
        sums = jnp.dot(
            jnp.concatenate([high, middle, low], 0), same_head, preferred_element_type=f32
        )
        size = values.shape[0]
        return sums[:size] + sums[size : 2 * size] + sums[2 * size :]

    decay_low = jnp.tanh(turned(tokens, landed(decay_down_ref)[...])).astype(jnp.bfloat16)
    rate_low = turned(tokens, landed(rate_down_ref)[...]).astype(jnp.bfloat16)
    decay_pre = landed(decay_base_ref)[...] + jnp.dot(
        decay_low, landed(decay_up_ref)[...], preferred_element_type=f32
    )
    decay = jnp.exp(-(math.exp(-0.5) * jax.nn.sigmoid(decay_pre)))
    in_rate = jax.nn.sigmoid(
        landed(rate_base_ref)[...]
        + jnp.dot(rate_low, landed(rate_up_ref)[...], preferred_element_type=f32)
    )
    key_vecs = jnp.dot(tokens, landed(w_key_ref)[...], preferred_element_type=f32)
    recep = jnp.dot(tokens, landed(w_recep_ref)[...], preferred_element_type=f32)
    sums = over_head(
        jnp.concatenate([key_vecs * key_vecs, key_vecs * in_rate * recep, key_vecs * recep], 0)
    )
    scale = lax.rsqrt(sums[:row_count] + key_epsilon)
    removed_factor = scale * sums[row_count : 2 * row_count]
    value_factor = sums[2 * row_count :]
    for which, vectors in enumerate((decay * recep, key_vecs * scale)):
        for h in range(heads):
            pair = vectors[:, h // 2 * 128 : h // 2 * 128 + 128]
            query_ref[pl.ds(which * heads + h, row_count, stride=2 * heads), :] = (
                pair if h % 2 == 0 else pltpu.roll(pair, head_size, 1)
            )
    for t in range(row_count):
        if t % (row_count // chunks) == 0:
            landed(state_ref, t // (row_count // chunks))
        queries = query_ref[2 * heads * t : 2 * heads * (t + 1), :head_size].astype(jnp.bfloat16)
        matrix = state_ref[t].reshape(width, head_size).astype(jnp.bfloat16)
        answers = turned(queries, matrix)
        for pair in range(heads // 2):
            answer_ref[pair, 2 * heads * t : 2 * heads * (t + 1), :] = answers[
                :, pair * 128 : (pair + 1) * 128
            ]
    first_of_pair = lax.broadcasted_iota(jnp.int32, (row_count, 128), 1) < head_size

    def picked(which):
        pairs = []
        for pair in range(heads // 2):
            of_pair = answer_ref.at[pair]
            rows = [
                of_pair[pl.ds(which * heads + 2 * pair + i, row_count, stride=2 * heads), :]
                for i in range(2)
            ]
            pairs.append(jnp.where(first_of_pair, rows[0], rows[1]))
        return jnp.concatenate(pairs, 1)

    value_vecs = jnp.dot(tokens, landed(w_value_ref)[...], preferred_element_type=f32)
    read_out = picked(0) - picked(1) * removed_factor + value_vecs * value_factor
    centred = read_out - over_head(read_out) * (1.0 / head_size)
    spread = over_head(centred * centred) * (1.0 / head_size)
    normed = centred * lax.rsqrt(spread + head_epsilon) * landed(head_gain_ref)[...]
    mixed = jnp.dot(normed.astype(jnp.bfloat16), landed(w_out_ref)[...], preferred_element_type=f32)
    mixed = mixed.astype(jnp.bfloat16)
    copies_out, mix_rows = message_ref.shape[0], row_count * heads
    landed(down_ref)
    for c in range(copies_out):
        for h in range(mixed.shape[1] // width):
            message_ref[c, h * row_count : (h + 1) * row_count, :] = mixed[
                :, h * width : (h + 1) * width
            ]
        message_ref[c, mix_rows:, :] = jnp.zeros_like(message_ref[c, mix_rows:, :])
        message_ref[c, mix_rows : mix_rows + down_ref.shape[0], :] = down_ref[...]


def mixer_message(
    copies_out,
    own_down,
    tokens,
    state,
    w_recep,
    w_key,
    w_value,
    w_out,
    decay_base,
    decay_down,
    decay_up,
    rate_base,
    rate_down,
    rate_up,
    head_gain,
):
    row_count, heads, head_size = state.shape[0], state.shape[1], state.shape[3]
    width = heads * head_size
    far = [
        tokens,
        decay_down.T,
        rate_down.T,
        decay_up,
        decay_base[None],
        rate_up,
        rate_base[None],
        w_key,
        w_recep,
        state,
        w_value,
        head_gain[None],
        w_out,
        own_down,
    ]
    chunks = 1
    down_rows = own_down.shape[0] + -own_down.shape[0] % 8
    rows = tokens.shape[1] // width * row_count + down_rows
    return pl.pallas_call(
        partial(mixer_kernel, chunks=chunks),
        out_shape=pltpu.VMEM((copies_out, rows, width), jnp.bfloat16),
        in_specs=[pl.BlockSpec(memory_space=pl.ANY)] * len(far),
        out_specs=pl.BlockSpec(memory_space=pltpu.VMEM),
        scratch_shapes=[pltpu.VMEM(a.shape, a.dtype) for a in far]
        + [
            pltpu.VMEM((2 * heads * row_count, 128), jnp.float32),
            pltpu.VMEM((heads // 2, 2 * heads * row_count, 128), jnp.float32),
            pltpu.SemaphoreType.DMA((len(far) - 1 + chunks,)),
        ],
        name="mixer",
    )(*far)


def expert_kernel(
    rows_ref, units_ref, gate_ref, up_ref, down_any, out_ref, down_ref, arrival, *, rows
):
    copies = [
        pltpu.make_async_copy(source, target, arrival.at[i])
        for i, (source, target) in enumerate(((down_any, down_ref),))
    ]
    for copy in copies:
        copy.start()
    blocks, splits, height, quarter = rows_ref.shape
    width = splits * quarter
    f32 = jnp.float32

    def turned(a, b):
        return lax.dot_general(a, b, (((1,), (1,)), ((), ())), preferred_element_type=f32)

    def whole_rows(low, high):
        return jnp.concatenate(
            [
                rows_ref[:, i, low:high, :].reshape(blocks * (high - low), quarter)
                for i in range(splits)
            ],
            1,
        )

    @pl.when(lax.axis_index("tp") >= 0)
    def _():
        dense = whole_rows(rows, height)
        gate_pre = turned(dense, units_ref[:, :width])
        up_pre = turned(dense, units_ref[:, width : 2 * width])
        hidden = (jax.nn.silu(gate_pre) * up_pre).astype(jnp.bfloat16)
        for i in range(splits):
            down = units_ref[:, 2 * width + i * quarter : 2 * width + (i + 1) * quarter]
            part = jnp.dot(hidden, down, preferred_element_type=f32).astype(jnp.bfloat16)
            out_ref[:, i, rows:, :] = part.reshape(blocks, height - rows, quarter)

    routed = whole_rows(0, rows)
    gate_pre = turned(routed, gate_ref[...])
    up_pre = turned(routed, up_ref[...])
    hidden = (jax.nn.silu(gate_pre) * up_pre).astype(jnp.bfloat16)
    copies[0].wait()
    for i in range(splits):
        down = down_ref[:, i * quarter : (i + 1) * quarter]
        part = jnp.dot(hidden, down, preferred_element_type=f32).astype(jnp.bfloat16)
        out_ref[:, i, :rows, :] = part.reshape(blocks, rows, quarter)


def run_experts(everything, units, expert_gate, expert_up, expert_down, rows):
    vmem = pl.BlockSpec(memory_space=pltpu.VMEM)
    held = [everything, units, expert_gate.T, expert_up.T]
    far = [expert_down]
    return pl.pallas_call(
        partial(expert_kernel, rows=rows),
        out_shape=pltpu.VMEM(everything.shape, jnp.bfloat16),
        in_specs=[vmem] * len(held) + [pl.BlockSpec(memory_space=pl.ANY)] * len(far),
        out_specs=vmem,
        scratch_shapes=[pltpu.VMEM(a.shape, a.dtype) for a in far]
        + [pltpu.SemaphoreType.DMA((len(far),))],
        input_output_aliases={0: 0},
        name="experts",
    )(*[on_chip(a) for a in held], *far)


def on_chip(value):
    return pltpu.with_memory_space_constraint(value, pltpu.VMEM)


def norm_kernel(
    everyone_ref,
    tokens_ref,
    gain_ref,
    branch_gate_ref,
    routes_ref,
    route_weights_ref,
    packed_ref,
    own_ref,
    factors_ref,
    *,
    experts,
    capacity,
    slots,
    shared,
):
    splits, _, quarter = everyone_ref.shape
    row_count = tokens_ref.shape[0]
    f32, i32 = jnp.float32, jnp.int32
    mixed = everyone_ref[0, : splits * row_count, :].astype(f32)
    for s in range(1, splits):
        mixed = mixed + everyone_ref[s, : splits * row_count, :].astype(f32)
    mixed = jnp.concatenate(
        [mixed[i * row_count : (i + 1) * row_count] for i in range(splits)], 1
    )
    x_mid = first_norm(residual_scale * tokens_ref[...].astype(f32) + mixed, gain_ref[...])
    own = jnp.zeros((row_count, quarter), f32)
    for i in range(splits):
        columns = x_mid[:, i * quarter : (i + 1) * quarter].astype(f32)
        own = jnp.where(lax.axis_index("tp") == i, columns, own)
    own_ref[...] = own
    branch = jax.nn.sigmoid(
        lax.dot_general(
            branch_gate_ref[...], x_mid, (((1,), (1,)), ((), ())), preferred_element_type=f32
        )
    )
    first, second = routes_ref[0:1, :], routes_ref[1:2, :]
    expert = lax.broadcasted_iota(i32, (experts, row_count), 0)
    hit_first, hit_second = (expert == first).astype(f32), (expert == second).astype(f32)
    before = (
        lax.broadcasted_iota(i32, (row_count, row_count), 0)
        < lax.broadcasted_iota(i32, (row_count, row_count), 1)
    ).astype(f32)
    earlier = jnp.dot(hit_first + hit_second, before, preferred_element_type=f32)
    slot_first = jnp.sum(earlier * hit_first, 0, keepdims=True).astype(i32)
    slot_second = jnp.sum(earlier * hit_second, 0, keepdims=True).astype(i32)
    lines = packed_ref.shape[0]
    height = lines * slots // (experts * capacity)
    place = lax.broadcasted_iota(i32, (lines, row_count), 0)
    row = lax.broadcasted_iota(i32, (lines, row_count), 1)
    plane, inner = place // height, place % height
    routed_place = jnp.where(inner < slots, plane * slots + inner, -1)
    dense_place = jnp.where(
        inner < slots, -1, plane % shared * (height - slots) + inner - slots
    )
    at_first = routed_place == first * capacity + slot_first
    at_second = routed_place == second * capacity + slot_second
    at_row = dense_place == row
    chosen = (at_first | at_second | at_row).astype(jnp.bfloat16)
    packed_ref[...] = jnp.dot(
        chosen, own.astype(jnp.bfloat16), preferred_element_type=f32
    ).astype(jnp.bfloat16)
    factors = (
        jnp.where(at_first, route_weights_ref[0:1, :], 0.0)
        + jnp.where(at_second, route_weights_ref[1:2, :], 0.0)
        + jnp.where(at_row, branch, 0.0)
    )
    factors_ref[...] = factors


def norm_and_pack(
    everyone,
    tokens,
    first_gain,
    branch_gate,
    routes,
    route_weights,
    lines,
    experts,
    capacity,
    slots,
    shared,
):
    row_count, quarter = tokens.shape[0], everyone.shape[2]
    vmem = pl.BlockSpec(memory_space=pltpu.VMEM)
    return pl.pallas_call(
        partial(norm_kernel, experts=experts, capacity=capacity, slots=slots, shared=shared),
        out_shape=(
            pltpu.VMEM((lines, quarter), jnp.bfloat16),
            pltpu.VMEM((row_count, quarter), jnp.float32),
            pltpu.VMEM((lines, row_count), jnp.float32),
        ),
        in_specs=[vmem] * 6,
        out_specs=(vmem, vmem, vmem),
        name="norm_and_pack",
    )(
        on_chip(everyone),
        on_chip(tokens),
        on_chip(first_gain[None]),
        on_chip(branch_gate[None]),
        on_chip(routes.T),
        on_chip(route_weights.T),
    )


def fan_choice(planes, slots_part, capacity, here, splits, shared):
    part = slots_part - here * capacity
    rows = planes * capacity
    index = np.arange(rows + shared * part)
    choice = np.zeros((here, splits, len(index), planes * slots_part), np.float32)
    for e in range(here):
        for i in range(splits):
            dense = index - rows
            routed_from = index // capacity * slots_part + e * capacity + index % capacity
            dense_from = (
                (i * shared + dense // part) * slots_part + here * capacity + dense % part
            )
            choice[e, i, index, np.where(index < rows, routed_from, dense_from)] = 1
    return choice.reshape(here * splits * len(index), planes * slots_part)


def fan_kernel(arrived_ref, choice_ref, out_any, laid_ref, sent):
    planes, slots_part, quarter = arrived_ref.shape
    here, copies, splits, height, _ = out_any.shape
    arrived = arrived_ref[...].reshape(planes * slots_part, quarter)
    started = []
    for e in range(here):
        size = splits * height
        laid = jnp.dot(
            choice_ref[e * size : (e + 1) * size, :], arrived, preferred_element_type=jnp.float32
        ).astype(jnp.bfloat16)
        for c in range(copies):
            laid_ref[e, c] = laid.reshape(splits, height, quarter)
        started.append(pltpu.make_async_copy(laid_ref.at[e], out_any.at[e], sent.at[e]))
        started[e].start()
    for copy in started:
        copy.wait()


def fan_out(arrived, capacity, here, copies, splits, shared):
    planes, slots_part, quarter = arrived.shape
    choice = fan_choice(planes, slots_part, capacity, here, splits, shared)
    height = choice.shape[0] // (here * splits)
    vmem = pl.BlockSpec(memory_space=pltpu.VMEM)
    shape = (here, copies, splits, height, quarter)
    return pl.pallas_call(
        fan_kernel,
        out_shape=jax.ShapeDtypeStruct(shape, jnp.bfloat16),
        in_specs=[vmem, vmem],
        out_specs=pl.BlockSpec(memory_space=pl.ANY),
        scratch_shapes=[pltpu.VMEM(shape, jnp.bfloat16), pltpu.SemaphoreType.DMA((here,))],
        name="fan_out",
    )(on_chip(arrived), on_chip(jnp.asarray(choice, jnp.bfloat16)))


def gather_kernel(returned_ref, out_ref, *, capacity, here, splits, shared):
    planes, slots_part, quarter = out_ref.shape
    sources, height, _ = returned_ref.shape
    part = slots_part - here * capacity
    rows = planes * capacity
    f32 = jnp.float32
    routed = []
    for e in range(here):
        total = jnp.zeros((rows, quarter), f32)
        for s in range(e * (sources // here), (e + 1) * (sources // here)):
            total = total + returned_ref[s, :rows, :].astype(f32)
        routed.append(total)
    dense = []
    for i in range(splits):
        total = jnp.zeros((height - rows, quarter), f32)
        for s in range(i, sources, splits):
            total = total + returned_ref[s, rows:, :].astype(f32)
        dense.append(total)
    sums = jnp.concatenate(routed + dense, 0).astype(jnp.bfloat16)
    shape = (planes * slots_part, sums.shape[0])
    line = lax.broadcasted_iota(jnp.int32, shape, 0)
    column = lax.broadcasted_iota(jnp.int32, shape, 1)
    z, inner = line // slots_part, line % slots_part
    routed_from = inner // capacity * rows + z * capacity + inner % capacity
    dense_from = here * rows + z * part + inner - here * capacity
    chosen = (
        column == jnp.where(inner < here * capacity, routed_from, dense_from)
    ).astype(jnp.bfloat16)
    laid = jnp.dot(chosen, sums, preferred_element_type=f32).astype(jnp.bfloat16)
    out_ref[...] = laid.reshape(planes, slots_part, quarter)


def gather_back(returned, planes, slots_part, capacity, here, splits, shared):
    vmem = pl.BlockSpec(memory_space=pltpu.VMEM)
    return pl.pallas_call(
        partial(gather_kernel, capacity=capacity, here=here, splits=splits, shared=shared),
        out_shape=pltpu.VMEM((planes, slots_part, returned.shape[2]), jnp.bfloat16),
        in_specs=[vmem],
        out_specs=vmem,
        name="gather_back",
    )(on_chip(returned))


def first_norm(values, gain):
    centre = jnp.mean(values, -1, keepdims=True)
    spread = jnp.mean(jnp.square(values - centre), -1, keepdims=True)
    return ((values - centre) * lax.rsqrt(spread + norm_epsilon) * gain).astype(jnp.bfloat16)


def shards(
    tokens,
    state,
    w_recep,
    w_key,
    w_value,
    w_out,
    decay_base,
    decay_down,
    decay_up,
    rate_base,
    rate_down,
    rate_up,
    head_gain,
    first_gain,
    expert_gate,
    expert_up,
    expert_down,
    dense_gate,
    dense_up,
    dense_down,
    branch_gate,
    second_gain,
    routes,
    route_weights,
):
    row_count = tokens.shape[0]
    model_width = tokens.shape[1]
    quarter = w_recep.shape[1]
    planes = lax.axis_size("z")
    plane_blocks = lax.axis_size(("x", "c"))
    plane_size = lax.axis_size(PLANE)
    tp_size = lax.axis_size("tp")
    shared = planes // tp_size
    message = mixer_message(
        tp_size,
        dense_down,
        tokens,
        state,
        w_recep,
        w_key,
        w_value,
        w_out,
        decay_base,
        decay_down,
        decay_up,
        rate_base,
        rate_down,
        rate_up,
        head_gain,
    )
    everyone = exchange(message, "tp")
    everyone, dense_gate, dense_up, branch_gate, expert_gate, expert_up, expert_down = (
        lax.optimization_barrier(
            (everyone, dense_gate, dense_up, branch_gate, expert_gate, expert_up, expert_down)
        )
    )
    mix_rows = tp_size * row_count
    units = jnp.concatenate(
        [padded_units(dense_gate, 8), padded_units(dense_up, 8)]
        + [everyone[i, mix_rows:] for i in range(tp_size)],
        1,
    )
    units = with_neighbour(units, 2)
    units = with_neighbour(units, 1)
    experts = lax.axis_size(EP) // SPLIT
    here = experts // planes
    capacity = min(row_count, max(2, 2 * row_count * routes.shape[1] // experts))
    slots = here * capacity
    part = row_count // shared
    packed_rows, own_columns, factors = norm_and_pack(
        everyone,
        tokens,
        first_gain,
        branch_gate,
        routes,
        route_weights,
        planes * (slots + part),
        experts,
        capacity,
        slots,
        shared,
    )
    arrived = exchange(packed_rows.reshape(planes, slots + part, quarter), "z")
    rows = planes * capacity
    dense_count = shared * part
    height = rows + dense_count
    outgoing = fan_out(arrived, capacity, here, plane_blocks // here, tp_size, shared)
    everything = exchange(outgoing.reshape(plane_size, height, quarter), PLANE)
    everything = everything.reshape(plane_blocks, tp_size, height, quarter)
    returning = run_experts(
        everything, units, expert_gate[0], expert_up[0], expert_down[0], rows
    )
    returned = exchange(returning.reshape(plane_size, height, quarter), PLANE)
    back = gather_back(returned, planes, slots + part, capacity, here, tp_size, shared)
    back = exchange(back, "z").reshape(planes * (slots + part), quarter)
    second_sum = residual_scale * own_columns + lax.dot_general(
        factors,
        back.astype(jnp.float32),
        (((0,), (0,)), ((), ())),
        precision=lax.Precision.HIGHEST,
        preferred_element_type=jnp.float32,
    )
    row_sums, square_sums = in_one(
        (jnp.sum(second_sum, 1), jnp.sum(second_sum * second_sum, 1)), "tp"
    )
    average = row_sums / model_width
    spread = square_sums / model_width - average * average
    return (
        (second_sum - average[:, None]) * lax.rsqrt(spread + norm_epsilon)[:, None] * second_gain
    ).astype(jnp.bfloat16)


def solution(mesh):
    finer = Mesh(mesh.devices.reshape(16, 4, 2, mesh.shape["tp"]), ("z", "x", "c", "tp"))
    return jax.shard_map(
        shards,
        mesh=finer,
        in_specs=(
            P(EP, None),
            P(EP, "tp", None, None),
            P(None, "tp"),
            P(None, "tp"),
            P(None, "tp"),
            P("tp", None),
            P("tp"),
            P(),
            P(None, "tp"),
            P("tp"),
            P(),
            P(None, "tp"),
            P("tp"),
            P(),
            P(EP, None, "tp"),
            P(EP, None, "tp"),
            P(EP, "tp", None),
            P(EP, None),
            P(EP, None),
            P(EP, "tp"),
            P(),
            P("tp"),
            P(EP, None),
            P(EP, None),
        ),
        out_specs=P(EP, "tp"),
        check_vma=False,
    )
```

```python
import math
from functools import partial

import jax
import jax.numpy as jnp
import numpy as np
from jax import lax
from jax.experimental import pallas as pl
from jax.experimental.pallas import tpu as pltpu
from jax.sharding import Mesh
from jax.sharding import PartitionSpec as P


SPLIT = 4
EP = ("z", "x", "c")
PLANE = ("x", "c", "tp")


residual_scale = 1.4142135623730951
norm_epsilon = 1e-05
head_epsilon = 0.00064
key_epsilon = 1e-06


def sent_to_all(value, axis):
    copies = jnp.broadcast_to(value, (lax.axis_size(axis), *value.shape))
    return lax.all_to_all(copies, axis, split_axis=0, concat_axis=0, tiled=True)


def of_everyone(value, axis):
    return sent_to_all(value, axis).astype(jnp.float32).sum(axis=0)


def exchange(parts, axis):
    return lax.all_to_all(parts, axis, split_axis=0, concat_axis=0, tiled=True)


def in_one(arrays, axis):
    vector, at, done = (jnp.concatenate([a.reshape(-1) for a in arrays]), 0, [])
    running = of_everyone(vector, axis)
    for a in arrays:
        done.append(running[at : at + a.size].reshape(a.shape))
        at += a.size
    return tuple(done)


def padded_units(columns, multiple):
    return jnp.pad(columns, ((0, -columns.shape[0] % multiple), (0, 0)))


def with_neighbour(units, step):
    planes = lax.axis_size("z")
    other = lax.ppermute(units, "z", [(i, i ^ step) for i in range(planes)])
    return jnp.concatenate([units, other], 0)


def mixer_kernel(*refs, groups):
    count = sum(groups)
    sources, message_ref = refs[:count], refs[count]
    targets = refs[count + 1 : count + 1 + len(groups)]
    query_ref, answer_ref, arrival = refs[count + 1 + len(groups) :]
    tokens_ref, low_ref, up_ref, base_ref, w_ref, state_ref, gain_ref, w_out_ref, down_ref = targets
    at = 0
    for group, (target, members) in enumerate(zip(targets, groups)):
        for i in range(members):
            part = target if members == 1 else target.at[i]
            pltpu.make_async_copy(sources[at], part, arrival.at[group]).start()
            at += 1

    def landed(target):
        group = [i for i, other in enumerate(targets) if other is target][0]
        pltpu.make_async_copy(target, target, arrival.at[group]).wait()
        return target

    row_count, heads, head_size = state_ref.shape[0], state_ref.shape[1], state_ref.shape[3]
    width = heads * head_size
    tokens = landed(tokens_ref)[...]
    f32 = jnp.float32

    def turned(a, b):
        return lax.dot_general(a, b, (((1,), (1,)), ((), ())), preferred_element_type=f32)

    channel_head = lax.broadcasted_iota(jnp.int32, (width, width), 0) // head_size
    same_head = (
        channel_head == lax.broadcasted_iota(jnp.int32, (width, width), 1) // head_size
    ).astype(jnp.bfloat16)

    def over_head(values):
        high = values.astype(jnp.bfloat16)
        rest = values - high.astype(f32)
        middle = rest.astype(jnp.bfloat16)
        low = (rest - middle.astype(f32)).astype(jnp.bfloat16)
        sums = jnp.dot(
            jnp.concatenate([high, middle, low], 0), same_head, preferred_element_type=f32
        )
        size = values.shape[0]
        return sums[:size] + sums[size : 2 * size] + sums[2 * size :]

    decay_low = jnp.tanh(turned(tokens, landed(low_ref)[0])).astype(jnp.bfloat16)
    rate_low = turned(tokens, low_ref[1]).astype(jnp.bfloat16)
    decay_pre = landed(base_ref)[0] + jnp.dot(
        decay_low, landed(up_ref)[0], preferred_element_type=f32
    )
    decay = jnp.exp(-(math.exp(-0.5) * jax.nn.sigmoid(decay_pre)))
    in_rate = jax.nn.sigmoid(
        base_ref[1]
        + jnp.dot(rate_low, up_ref[1], preferred_element_type=f32)
    )
    key_vecs = jnp.dot(tokens, landed(w_ref)[0], preferred_element_type=f32)
    recep = jnp.dot(tokens, w_ref[1], preferred_element_type=f32)
    sums = over_head(
        jnp.concatenate([key_vecs * key_vecs, key_vecs * in_rate * recep, key_vecs * recep], 0)
    )
    scale = lax.rsqrt(sums[:row_count] + key_epsilon)
    removed_factor = scale * sums[row_count : 2 * row_count]
    value_factor = sums[2 * row_count :]
    for which, vectors in enumerate((decay * recep, key_vecs * scale)):
        for h in range(heads):
            pair = vectors[:, h // 2 * 128 : h // 2 * 128 + 128]
            query_ref[pl.ds(which * heads + h, row_count, stride=2 * heads), :] = (
                pair if h % 2 == 0 else pltpu.roll(pair, head_size, 1)
            )
    landed(state_ref)
    for t in range(row_count):
        queries = query_ref[2 * heads * t : 2 * heads * (t + 1), :head_size].astype(jnp.bfloat16)
        matrix = state_ref[t].reshape(width, head_size).astype(jnp.bfloat16)
        answers = turned(queries, matrix)
        for pair in range(heads // 2):
            answer_ref[pair, 2 * heads * t : 2 * heads * (t + 1), :] = answers[
                :, pair * 128 : (pair + 1) * 128
            ]
    first_of_pair = lax.broadcasted_iota(jnp.int32, (row_count, 128), 1) < head_size

    def picked(which):
        pairs = []
        for pair in range(heads // 2):
            of_pair = answer_ref.at[pair]
            rows = [
                of_pair[pl.ds(which * heads + 2 * pair + i, row_count, stride=2 * heads), :]
                for i in range(2)
            ]
            pairs.append(jnp.where(first_of_pair, rows[0], rows[1]))
        return jnp.concatenate(pairs, 1)

    value_vecs = jnp.dot(tokens, w_ref[2], preferred_element_type=f32)
    read_out = picked(0) - picked(1) * removed_factor + value_vecs * value_factor
    centred = read_out - over_head(read_out) * (1.0 / head_size)
    spread = over_head(centred * centred) * (1.0 / head_size)
    normed = centred * lax.rsqrt(spread + head_epsilon) * landed(gain_ref)[...]
    mixed = jnp.dot(normed.astype(jnp.bfloat16), landed(w_out_ref)[...], preferred_element_type=f32)
    mixed = mixed.astype(jnp.bfloat16)
    copies_out, mix_rows = message_ref.shape[0], row_count * heads
    landed(down_ref)
    for c in range(copies_out):
        for h in range(mixed.shape[1] // width):
            message_ref[c, h * row_count : (h + 1) * row_count, :] = mixed[
                :, h * width : (h + 1) * width
            ]
        message_ref[c, mix_rows:, :] = jnp.zeros_like(message_ref[c, mix_rows:, :])
        message_ref[c, mix_rows : mix_rows + down_ref.shape[0], :] = down_ref[...]


def mixer_message(
    copies_out,
    own_down,
    tokens,
    state,
    w_recep,
    w_key,
    w_value,
    w_out,
    decay_base,
    decay_down,
    decay_up,
    rate_base,
    rate_down,
    rate_up,
    head_gain,
):
    row_count, heads, head_size = state.shape[0], state.shape[1], state.shape[3]
    width = heads * head_size
    far = [
        [tokens],
        [decay_down.T, rate_down.T],
        [decay_up, rate_up],
        [decay_base[None], rate_base[None]],
        [w_key, w_recep, w_value],
        [state],
        [head_gain[None]],
        [w_out],
        [own_down],
    ]
    down_rows = own_down.shape[0] + -own_down.shape[0] % 8
    rows = tokens.shape[1] // width * row_count + down_rows
    return pl.pallas_call(
        partial(mixer_kernel, groups=[len(group) for group in far]),
        out_shape=pltpu.VMEM((copies_out, rows, width), jnp.bfloat16),
        in_specs=[pl.BlockSpec(memory_space=pl.ANY)] * sum(len(group) for group in far),
        out_specs=pl.BlockSpec(memory_space=pltpu.VMEM),
        scratch_shapes=[
            pltpu.VMEM((len(g), *g[0].shape) if len(g) > 1 else g[0].shape, g[0].dtype)
            for g in far
        ]
        + [
            pltpu.VMEM((2 * heads * row_count, 128), jnp.float32),
            pltpu.VMEM((heads // 2, 2 * heads * row_count, 128), jnp.float32),
            pltpu.SemaphoreType.DMA((len(far),)),
        ],
        name="mixer",
    )(*[a for group in far for a in group])


def expert_kernel(
    rows_ref, units_ref, gate_ref, up_ref, down_any, out_ref, down_ref, arrival, *, rows
):
    copies = [
        pltpu.make_async_copy(source, target, arrival.at[i])
        for i, (source, target) in enumerate(((down_any, down_ref),))
    ]
    for copy in copies:
        copy.start()
    blocks, splits, height, quarter = rows_ref.shape
    width = splits * quarter
    f32 = jnp.float32

    def turned(a, b):
        return lax.dot_general(a, b, (((1,), (1,)), ((), ())), preferred_element_type=f32)

    def whole_rows(low, high):
        return jnp.concatenate(
            [
                rows_ref[:, i, low:high, :].reshape(blocks * (high - low), quarter)
                for i in range(splits)
            ],
            1,
        )

    @pl.when(lax.axis_index("tp") >= 0)
    def _():
        dense = whole_rows(rows, height)
        gate_pre = turned(dense, units_ref[:, :width])
        up_pre = turned(dense, units_ref[:, width : 2 * width])
        hidden = (jax.nn.silu(gate_pre) * up_pre).astype(jnp.bfloat16)
        for i in range(splits):
            down = units_ref[:, 2 * width + i * quarter : 2 * width + (i + 1) * quarter]
            part = jnp.dot(hidden, down, preferred_element_type=f32).astype(jnp.bfloat16)
            out_ref[:, i, rows:, :] = part.reshape(blocks, height - rows, quarter)

    routed = whole_rows(0, rows)
    gate_pre = turned(routed, gate_ref[...])
    up_pre = turned(routed, up_ref[...])
    hidden = (jax.nn.silu(gate_pre) * up_pre).astype(jnp.bfloat16)
    copies[0].wait()
    for i in range(splits):
        down = down_ref[:, i * quarter : (i + 1) * quarter]
        part = jnp.dot(hidden, down, preferred_element_type=f32).astype(jnp.bfloat16)
        out_ref[:, i, :rows, :] = part.reshape(blocks, rows, quarter)


def run_experts(everything, units, expert_gate, expert_up, expert_down, rows):
    vmem = pl.BlockSpec(memory_space=pltpu.VMEM)
    held = [everything, units, expert_gate.T, expert_up.T]
    far = [expert_down]
    return pl.pallas_call(
        partial(expert_kernel, rows=rows),
        out_shape=pltpu.VMEM(everything.shape, jnp.bfloat16),
        in_specs=[vmem] * len(held) + [pl.BlockSpec(memory_space=pl.ANY)] * len(far),
        out_specs=vmem,
        scratch_shapes=[pltpu.VMEM(a.shape, a.dtype) for a in far]
        + [pltpu.SemaphoreType.DMA((len(far),))],
        input_output_aliases={0: 0},
        name="experts",
    )(*[on_chip(a) for a in held], *far)


def on_chip(value):
    return pltpu.with_memory_space_constraint(value, pltpu.VMEM)


def norm_kernel(
    everyone_ref,
    tokens_ref,
    gain_ref,
    branch_gate_ref,
    routes_ref,
    route_weights_ref,
    packed_ref,
    own_ref,
    factors_ref,
    *,
    experts,
    capacity,
    slots,
    shared,
):
    splits, _, quarter = everyone_ref.shape
    row_count = tokens_ref.shape[0]
    f32, i32 = jnp.float32, jnp.int32
    mixed = everyone_ref[0, : splits * row_count, :].astype(f32)
    for s in range(1, splits):
        mixed = mixed + everyone_ref[s, : splits * row_count, :].astype(f32)
    mixed = jnp.concatenate(
        [mixed[i * row_count : (i + 1) * row_count] for i in range(splits)], 1
    )
    x_mid = first_norm(residual_scale * tokens_ref[...].astype(f32) + mixed, gain_ref[...])
    own = jnp.zeros((row_count, quarter), f32)
    for i in range(splits):
        columns = x_mid[:, i * quarter : (i + 1) * quarter].astype(f32)
        own = jnp.where(lax.axis_index("tp") == i, columns, own)
    own_ref[...] = own
    branch = jax.nn.sigmoid(
        lax.dot_general(
            branch_gate_ref[...], x_mid, (((1,), (1,)), ((), ())), preferred_element_type=f32
        )
    )
    first, second = routes_ref[0:1, :], routes_ref[1:2, :]
    expert = lax.broadcasted_iota(i32, (experts, row_count), 0)
    hit_first, hit_second = (expert == first).astype(f32), (expert == second).astype(f32)
    before = (
        lax.broadcasted_iota(i32, (row_count, row_count), 0)
        < lax.broadcasted_iota(i32, (row_count, row_count), 1)
    ).astype(f32)
    earlier = jnp.dot(hit_first + hit_second, before, preferred_element_type=f32)
    slot_first = jnp.sum(earlier * hit_first, 0, keepdims=True).astype(i32)
    slot_second = jnp.sum(earlier * hit_second, 0, keepdims=True).astype(i32)
    lines = packed_ref.shape[0]
    height = lines * slots // (experts * capacity)
    place = lax.broadcasted_iota(i32, (lines, row_count), 0)
    row = lax.broadcasted_iota(i32, (lines, row_count), 1)
    plane, inner = place // height, place % height
    routed_place = jnp.where(inner < slots, plane * slots + inner, -1)
    dense_place = jnp.where(
        inner < slots, -1, plane % shared * (height - slots) + inner - slots
    )
    at_first = routed_place == first * capacity + slot_first
    at_second = routed_place == second * capacity + slot_second
    at_row = dense_place == row
    chosen = (at_first | at_second | at_row).astype(jnp.bfloat16)
    packed_ref[...] = jnp.dot(
        chosen, own.astype(jnp.bfloat16), preferred_element_type=f32
    ).astype(jnp.bfloat16)
    factors = (
        jnp.where(at_first, route_weights_ref[0:1, :], 0.0)
        + jnp.where(at_second, route_weights_ref[1:2, :], 0.0)
        + jnp.where(at_row, branch, 0.0)
    )
    factors_ref[...] = factors


def norm_and_pack(
    everyone,
    tokens,
    first_gain,
    branch_gate,
    routes,
    route_weights,
    lines,
    experts,
    capacity,
    slots,
    shared,
):
    row_count, quarter = tokens.shape[0], everyone.shape[2]
    vmem = pl.BlockSpec(memory_space=pltpu.VMEM)
    return pl.pallas_call(
        partial(norm_kernel, experts=experts, capacity=capacity, slots=slots, shared=shared),
        out_shape=(
            pltpu.VMEM((lines, quarter), jnp.bfloat16),
            pltpu.VMEM((row_count, quarter), jnp.float32),
            pltpu.VMEM((lines, row_count), jnp.float32),
        ),
        in_specs=[vmem] * 6,
        out_specs=(vmem, vmem, vmem),
        name="norm_and_pack",
    )(
        on_chip(everyone),
        on_chip(tokens),
        on_chip(first_gain[None]),
        on_chip(branch_gate[None]),
        on_chip(routes.T),
        on_chip(route_weights.T),
    )


def fan_choice(planes, slots_part, capacity, here, splits, shared):
    part = slots_part - here * capacity
    rows = planes * capacity
    index = np.arange(rows + shared * part)
    choice = np.zeros((here, splits, len(index), planes * slots_part), np.float32)
    for e in range(here):
        for i in range(splits):
            dense = index - rows
            routed_from = index // capacity * slots_part + e * capacity + index % capacity
            dense_from = (
                (i * shared + dense // part) * slots_part + here * capacity + dense % part
            )
            choice[e, i, index, np.where(index < rows, routed_from, dense_from)] = 1
    return choice.reshape(here * splits * len(index), planes * slots_part)


def fan_kernel(arrived_ref, choice_ref, out_any, laid_ref, sent):
    planes, slots_part, quarter = arrived_ref.shape
    here, copies, splits, height, _ = out_any.shape
    arrived = arrived_ref[...].reshape(planes * slots_part, quarter)
    started = []
    for e in range(here):
        size = splits * height
        laid = jnp.dot(
            choice_ref[e * size : (e + 1) * size, :], arrived, preferred_element_type=jnp.float32
        ).astype(jnp.bfloat16)
        for c in range(copies):
            laid_ref[e, c] = laid.reshape(splits, height, quarter)
        started.append(pltpu.make_async_copy(laid_ref.at[e], out_any.at[e], sent.at[e]))
        started[e].start()
    for copy in started:
        copy.wait()


def fan_out(arrived, capacity, here, copies, splits, shared):
    planes, slots_part, quarter = arrived.shape
    choice = fan_choice(planes, slots_part, capacity, here, splits, shared)
    height = choice.shape[0] // (here * splits)
    vmem = pl.BlockSpec(memory_space=pltpu.VMEM)
    shape = (here, copies, splits, height, quarter)
    return pl.pallas_call(
        fan_kernel,
        out_shape=jax.ShapeDtypeStruct(shape, jnp.bfloat16),
        in_specs=[vmem, vmem],
        out_specs=pl.BlockSpec(memory_space=pl.ANY),
        scratch_shapes=[pltpu.VMEM(shape, jnp.bfloat16), pltpu.SemaphoreType.DMA((here,))],
        name="fan_out",
    )(on_chip(arrived), on_chip(jnp.asarray(choice, jnp.bfloat16)))


def gather_kernel(returned_ref, out_ref, *, capacity, here, splits, shared):
    planes, slots_part, quarter = out_ref.shape
    sources, height, _ = returned_ref.shape
    part = slots_part - here * capacity
    rows = planes * capacity
    f32 = jnp.float32
    routed = []
    for e in range(here):
        total = jnp.zeros((rows, quarter), f32)
        for s in range(e * (sources // here), (e + 1) * (sources // here)):
            total = total + returned_ref[s, :rows, :].astype(f32)
        routed.append(total)
    dense = []
    for i in range(splits):
        total = jnp.zeros((height - rows, quarter), f32)
        for s in range(i, sources, splits):
            total = total + returned_ref[s, rows:, :].astype(f32)
        dense.append(total)
    sums = jnp.concatenate(routed + dense, 0).astype(jnp.bfloat16)
    shape = (planes * slots_part, sums.shape[0])
    line = lax.broadcasted_iota(jnp.int32, shape, 0)
    column = lax.broadcasted_iota(jnp.int32, shape, 1)
    z, inner = line // slots_part, line % slots_part
    routed_from = inner // capacity * rows + z * capacity + inner % capacity
    dense_from = here * rows + z * part + inner - here * capacity
    chosen = (
        column == jnp.where(inner < here * capacity, routed_from, dense_from)
    ).astype(jnp.bfloat16)
    laid = jnp.dot(chosen, sums, preferred_element_type=f32).astype(jnp.bfloat16)
    out_ref[...] = laid.reshape(planes, slots_part, quarter)


def gather_back(returned, planes, slots_part, capacity, here, splits, shared):
    vmem = pl.BlockSpec(memory_space=pltpu.VMEM)
    return pl.pallas_call(
        partial(gather_kernel, capacity=capacity, here=here, splits=splits, shared=shared),
        out_shape=pltpu.VMEM((planes, slots_part, returned.shape[2]), jnp.bfloat16),
        in_specs=[vmem],
        out_specs=vmem,
        name="gather_back",
    )(on_chip(returned))


def first_norm(values, gain):
    centre = jnp.mean(values, -1, keepdims=True)
    spread = jnp.mean(jnp.square(values - centre), -1, keepdims=True)
    return ((values - centre) * lax.rsqrt(spread + norm_epsilon) * gain).astype(jnp.bfloat16)


def shards(
    tokens,
    state,
    w_recep,
    w_key,
    w_value,
    w_out,
    decay_base,
    decay_down,
    decay_up,
    rate_base,
    rate_down,
    rate_up,
    head_gain,
    first_gain,
    expert_gate,
    expert_up,
    expert_down,
    dense_gate,
    dense_up,
    dense_down,
    branch_gate,
    second_gain,
    routes,
    route_weights,
):
    row_count = tokens.shape[0]
    model_width = tokens.shape[1]
    quarter = w_recep.shape[1]
    planes = lax.axis_size("z")
    plane_blocks = lax.axis_size(("x", "c"))
    plane_size = lax.axis_size(PLANE)
    tp_size = lax.axis_size("tp")
    shared = planes // tp_size
    message = mixer_message(
        tp_size,
        dense_down,
        tokens,
        state,
        w_recep,
        w_key,
        w_value,
        w_out,
        decay_base,
        decay_down,
        decay_up,
        rate_base,
        rate_down,
        rate_up,
        head_gain,
    )
    everyone = exchange(message, "tp")
    everyone, dense_gate, dense_up, branch_gate, expert_gate, expert_up, expert_down = (
        lax.optimization_barrier(
            (everyone, dense_gate, dense_up, branch_gate, expert_gate, expert_up, expert_down)
        )
    )
    mix_rows = tp_size * row_count
    units = jnp.concatenate(
        [padded_units(dense_gate, 8), padded_units(dense_up, 8)]
        + [everyone[i, mix_rows:] for i in range(tp_size)],
        1,
    )
    units = with_neighbour(units, 2)
    units = with_neighbour(units, 1)
    experts = lax.axis_size(EP) // SPLIT
    here = experts // planes
    capacity = min(row_count, max(2, 2 * row_count * routes.shape[1] // experts))
    slots = here * capacity
    part = row_count // shared
    packed_rows, own_columns, factors = norm_and_pack(
        everyone,
        tokens,
        first_gain,
        branch_gate,
        routes,
        route_weights,
        planes * (slots + part),
        experts,
        capacity,
        slots,
        shared,
    )
    arrived = exchange(packed_rows.reshape(planes, slots + part, quarter), "z")
    rows = planes * capacity
    dense_count = shared * part
    height = rows + dense_count
    outgoing = fan_out(arrived, capacity, here, plane_blocks // here, tp_size, shared)
    everything = exchange(outgoing.reshape(plane_size, height, quarter), PLANE)
    everything = everything.reshape(plane_blocks, tp_size, height, quarter)
    returning = run_experts(
        everything, units, expert_gate[0], expert_up[0], expert_down[0], rows
    )
    returned = exchange(returning.reshape(plane_size, height, quarter), PLANE)
    back = gather_back(returned, planes, slots + part, capacity, here, tp_size, shared)
    back = exchange(back, "z").reshape(planes * (slots + part), quarter)
    second_sum = residual_scale * own_columns + lax.dot_general(
        factors,
        back.astype(jnp.float32),
        (((0,), (0,)), ((), ())),
        precision=lax.Precision.HIGHEST,
        preferred_element_type=jnp.float32,
    )
    row_sums, square_sums = in_one(
        (jnp.sum(second_sum, 1), jnp.sum(second_sum * second_sum, 1)), "tp"
    )
    average = row_sums / model_width
    spread = square_sums / model_width - average * average
    return (
        (second_sum - average[:, None]) * lax.rsqrt(spread + norm_epsilon)[:, None] * second_gain
    ).astype(jnp.bfloat16)


def solution(mesh):
    finer = Mesh(mesh.devices.reshape(16, 4, 2, mesh.shape["tp"]), ("z", "x", "c", "tp"))
    return jax.shard_map(
        shards,
        mesh=finer,
        in_specs=(
            P(EP, None),
            P(EP, "tp", None, None),
            P(None, "tp"),
            P(None, "tp"),
            P(None, "tp"),
            P("tp", None),
            P("tp"),
            P(),
            P(None, "tp"),
            P("tp"),
            P(),
            P(None, "tp"),
            P("tp"),
            P(),
            P(EP, None, "tp"),
            P(EP, None, "tp"),
            P(EP, "tp", None),
            P(EP, None),
            P(EP, None),
            P(EP, "tp"),
            P(),
            P("tp"),
            P(EP, None),
            P(EP, None),
        ),
        out_specs=P(EP, "tp"),
        check_vma=False,
    )
```

```python
import math
from functools import partial

import jax
import jax.numpy as jnp
import numpy as np
from jax import lax
from jax.experimental import pallas as pl
from jax.experimental.pallas import tpu as pltpu
from jax.sharding import Mesh
from jax.sharding import PartitionSpec as P


SPLIT = 4
EP = ("z", "x", "c")
PLANE = ("x", "c", "tp")


residual_scale = 1.4142135623730951
norm_epsilon = 1e-05
head_epsilon = 0.00064
key_epsilon = 1e-06


def sent_to_all(value, axis):
    copies = jnp.broadcast_to(value, (lax.axis_size(axis), *value.shape))
    return lax.all_to_all(copies, axis, split_axis=0, concat_axis=0, tiled=True)


def of_everyone(value, axis):
    return sent_to_all(value, axis).astype(jnp.float32).sum(axis=0)


def exchange(parts, axis):
    return lax.all_to_all(parts, axis, split_axis=0, concat_axis=0, tiled=True)


def in_one(arrays, axis):
    vector, at, done = (jnp.concatenate([a.reshape(-1) for a in arrays]), 0, [])
    running = of_everyone(vector, axis)
    for a in arrays:
        done.append(running[at : at + a.size].reshape(a.shape))
        at += a.size
    return tuple(done)


def padded_units(columns, multiple):
    return jnp.pad(columns, ((0, -columns.shape[0] % multiple), (0, 0)))


def with_neighbour(units, step):
    planes = lax.axis_size("z")
    other = lax.ppermute(units, "z", [(i, i ^ step) for i in range(planes)])
    return jnp.concatenate([units, other], 0)


def mixer_kernel(*refs, groups):
    count = sum(groups)
    sources, message_ref = refs[:count], refs[count]
    targets = refs[count + 1 : count + 1 + len(groups)]
    query_ref, answer_ref, arrival = refs[count + 1 + len(groups) :]
    tokens_ref, low_ref, up_ref, base_ref, w_ref, state_ref, w_out_ref, down_ref = targets
    at = 0
    for group, (target, members) in enumerate(zip(targets, groups)):
        for i in range(members):
            part = target if members == 1 else target.at[i]
            pltpu.make_async_copy(sources[at], part, arrival.at[group]).start()
            at += 1

    def landed(target):
        group = [i for i, other in enumerate(targets) if other is target][0]
        pltpu.make_async_copy(target, target, arrival.at[group]).wait()
        return target

    row_count, heads, head_size = state_ref.shape[0], state_ref.shape[1], state_ref.shape[3]
    width = heads * head_size
    tokens = landed(tokens_ref)[...]
    f32 = jnp.float32

    def turned(a, b):
        return lax.dot_general(a, b, (((1,), (1,)), ((), ())), preferred_element_type=f32)

    channel_head = lax.broadcasted_iota(jnp.int32, (width, width), 0) // head_size
    same_head = (
        channel_head == lax.broadcasted_iota(jnp.int32, (width, width), 1) // head_size
    ).astype(jnp.bfloat16)

    def over_head(values):
        high = values.astype(jnp.bfloat16)
        rest = values - high.astype(f32)
        middle = rest.astype(jnp.bfloat16)
        low = (rest - middle.astype(f32)).astype(jnp.bfloat16)
        sums = jnp.dot(
            jnp.concatenate([high, middle, low], 0), same_head, preferred_element_type=f32
        )
        size = values.shape[0]
        return sums[:size] + sums[size : 2 * size] + sums[2 * size :]

    decay_low = jnp.tanh(turned(tokens, landed(low_ref)[0])).astype(jnp.bfloat16)
    rate_low = turned(tokens, low_ref[1]).astype(jnp.bfloat16)
    decay_pre = landed(base_ref)[0] + jnp.dot(
        decay_low, landed(up_ref)[0], preferred_element_type=f32
    )
    decay = jnp.exp(-(math.exp(-0.5) * jax.nn.sigmoid(decay_pre)))
    in_rate = jax.nn.sigmoid(
        base_ref[1]
        + jnp.dot(rate_low, up_ref[1], preferred_element_type=f32)
    )
    key_vecs = jnp.dot(tokens, landed(w_ref)[0], preferred_element_type=f32)
    recep = jnp.dot(tokens, w_ref[1], preferred_element_type=f32)
    sums = over_head(
        jnp.concatenate([key_vecs * key_vecs, key_vecs * in_rate * recep, key_vecs * recep], 0)
    )
    scale = lax.rsqrt(sums[:row_count] + key_epsilon)
    removed_factor = scale * sums[row_count : 2 * row_count]
    value_factor = sums[2 * row_count :]
    for which, vectors in enumerate((decay * recep, key_vecs * scale)):
        for h in range(heads):
            pair = vectors[:, h // 2 * 128 : h // 2 * 128 + 128]
            query_ref[pl.ds(which * heads + h, row_count, stride=2 * heads), :] = (
                pair if h % 2 == 0 else pltpu.roll(pair, head_size, 1)
            )
    landed(state_ref)
    for t in range(row_count):
        queries = query_ref[2 * heads * t : 2 * heads * (t + 1), :head_size].astype(jnp.bfloat16)
        matrix = state_ref[t].reshape(width, head_size).astype(jnp.bfloat16)
        answers = turned(queries, matrix)
        for pair in range(heads // 2):
            answer_ref[pair, 2 * heads * t : 2 * heads * (t + 1), :] = answers[
                :, pair * 128 : (pair + 1) * 128
            ]
    first_of_pair = lax.broadcasted_iota(jnp.int32, (row_count, 128), 1) < head_size

    def picked(which):
        pairs = []
        for pair in range(heads // 2):
            of_pair = answer_ref.at[pair]
            rows = [
                of_pair[pl.ds(which * heads + 2 * pair + i, row_count, stride=2 * heads), :]
                for i in range(2)
            ]
            pairs.append(jnp.where(first_of_pair, rows[0], rows[1]))
        return jnp.concatenate(pairs, 1)

    value_vecs = jnp.dot(tokens, w_ref[2], preferred_element_type=f32)
    read_out = picked(0) - picked(1) * removed_factor + value_vecs * value_factor
    centred = read_out - over_head(read_out) * (1.0 / head_size)
    spread = over_head(centred * centred) * (1.0 / head_size)
    normed = centred * lax.rsqrt(spread + head_epsilon) * base_ref[2]
    mixed = jnp.dot(normed.astype(jnp.bfloat16), landed(w_out_ref)[...], preferred_element_type=f32)
    mixed = mixed.astype(jnp.bfloat16)
    copies_out, mix_rows = message_ref.shape[0], row_count * heads
    landed(down_ref)
    for c in range(copies_out):
        for h in range(mixed.shape[1] // width):
            message_ref[c, h * row_count : (h + 1) * row_count, :] = mixed[
                :, h * width : (h + 1) * width
            ]
        message_ref[c, mix_rows:, :] = jnp.zeros_like(message_ref[c, mix_rows:, :])
        message_ref[c, mix_rows : mix_rows + down_ref.shape[0], :] = down_ref[...]


def mixer_message(
    copies_out,
    own_down,
    tokens,
    state,
    w_recep,
    w_key,
    w_value,
    w_out,
    decay_base,
    decay_down,
    decay_up,
    rate_base,
    rate_down,
    rate_up,
    head_gain,
):
    row_count, heads, head_size = state.shape[0], state.shape[1], state.shape[3]
    width = heads * head_size
    far = [
        [tokens],
        [decay_down.T, rate_down.T],
        [decay_up, rate_up],
        [decay_base[None], rate_base[None], head_gain[None]],
        [w_key, w_recep, w_value],
        [state],
        [w_out],
        [own_down],
    ]
    down_rows = own_down.shape[0] + -own_down.shape[0] % 8
    rows = tokens.shape[1] // width * row_count + down_rows
    return pl.pallas_call(
        partial(mixer_kernel, groups=[len(group) for group in far]),
        out_shape=pltpu.VMEM((copies_out, rows, width), jnp.bfloat16),
        in_specs=[pl.BlockSpec(memory_space=pl.ANY)] * sum(len(group) for group in far),
        out_specs=pl.BlockSpec(memory_space=pltpu.VMEM),
        scratch_shapes=[
            pltpu.VMEM((len(g), *g[0].shape) if len(g) > 1 else g[0].shape, g[0].dtype)
            for g in far
        ]
        + [
            pltpu.VMEM((2 * heads * row_count, 128), jnp.float32),
            pltpu.VMEM((heads // 2, 2 * heads * row_count, 128), jnp.float32),
            pltpu.SemaphoreType.DMA((len(far),)),
        ],
        name="mixer",
    )(*[a for group in far for a in group])


def expert_kernel(
    rows_ref, units_ref, gate_ref, up_ref, down_any, out_ref, down_ref, arrival, *, rows
):
    copies = [
        pltpu.make_async_copy(source, target, arrival.at[i])
        for i, (source, target) in enumerate(((down_any, down_ref),))
    ]
    for copy in copies:
        copy.start()
    blocks, splits, height, quarter = rows_ref.shape
    width = splits * quarter
    f32 = jnp.float32

    def turned(a, b):
        return lax.dot_general(a, b, (((1,), (1,)), ((), ())), preferred_element_type=f32)

    def whole_rows(low, high):
        return jnp.concatenate(
            [
                rows_ref[:, i, low:high, :].reshape(blocks * (high - low), quarter)
                for i in range(splits)
            ],
            1,
        )

    @pl.when(lax.axis_index("tp") >= 0)
    def _():
        dense = whole_rows(rows, height)
        gate_pre = turned(dense, units_ref[:, :width])
        up_pre = turned(dense, units_ref[:, width : 2 * width])
        hidden = (jax.nn.silu(gate_pre) * up_pre).astype(jnp.bfloat16)
        for i in range(splits):
            down = units_ref[:, 2 * width + i * quarter : 2 * width + (i + 1) * quarter]
            part = jnp.dot(hidden, down, preferred_element_type=f32).astype(jnp.bfloat16)
            out_ref[:, i, rows:, :] = part.reshape(blocks, height - rows, quarter)

    routed = whole_rows(0, rows)
    gate_pre = turned(routed, gate_ref[...])
    up_pre = turned(routed, up_ref[...])
    hidden = (jax.nn.silu(gate_pre) * up_pre).astype(jnp.bfloat16)
    copies[0].wait()
    for i in range(splits):
        down = down_ref[:, i * quarter : (i + 1) * quarter]
        part = jnp.dot(hidden, down, preferred_element_type=f32).astype(jnp.bfloat16)
        out_ref[:, i, :rows, :] = part.reshape(blocks, rows, quarter)


def run_experts(everything, units, expert_gate, expert_up, expert_down, rows):
    vmem = pl.BlockSpec(memory_space=pltpu.VMEM)
    held = [everything, units, expert_gate.T, expert_up.T]
    far = [expert_down]
    return pl.pallas_call(
        partial(expert_kernel, rows=rows),
        out_shape=pltpu.VMEM(everything.shape, jnp.bfloat16),
        in_specs=[vmem] * len(held) + [pl.BlockSpec(memory_space=pl.ANY)] * len(far),
        out_specs=vmem,
        scratch_shapes=[pltpu.VMEM(a.shape, a.dtype) for a in far]
        + [pltpu.SemaphoreType.DMA((len(far),))],
        input_output_aliases={0: 0},
        name="experts",
    )(*[on_chip(a) for a in held], *far)


def on_chip(value):
    return pltpu.with_memory_space_constraint(value, pltpu.VMEM)


def norm_kernel(
    everyone_ref,
    tokens_ref,
    gain_ref,
    branch_gate_ref,
    routes_ref,
    route_weights_ref,
    packed_ref,
    own_ref,
    factors_ref,
    *,
    experts,
    capacity,
    slots,
    shared,
):
    splits, _, quarter = everyone_ref.shape
    row_count = tokens_ref.shape[0]
    f32, i32 = jnp.float32, jnp.int32
    mixed = everyone_ref[0, : splits * row_count, :].astype(f32)
    for s in range(1, splits):
        mixed = mixed + everyone_ref[s, : splits * row_count, :].astype(f32)
    mixed = jnp.concatenate(
        [mixed[i * row_count : (i + 1) * row_count] for i in range(splits)], 1
    )
    x_mid = first_norm(residual_scale * tokens_ref[...].astype(f32) + mixed, gain_ref[...])
    own = jnp.zeros((row_count, quarter), f32)
    for i in range(splits):
        columns = x_mid[:, i * quarter : (i + 1) * quarter].astype(f32)
        own = jnp.where(lax.axis_index("tp") == i, columns, own)
    own_ref[...] = own
    branch = jax.nn.sigmoid(
        lax.dot_general(
            branch_gate_ref[...], x_mid, (((1,), (1,)), ((), ())), preferred_element_type=f32
        )
    )
    first, second = routes_ref[0:1, :], routes_ref[1:2, :]
    expert = lax.broadcasted_iota(i32, (experts, row_count), 0)
    hit_first, hit_second = (expert == first).astype(f32), (expert == second).astype(f32)
    before = (
        lax.broadcasted_iota(i32, (row_count, row_count), 0)
        < lax.broadcasted_iota(i32, (row_count, row_count), 1)
    ).astype(f32)
    earlier = jnp.dot(hit_first + hit_second, before, preferred_element_type=f32)
    slot_first = jnp.sum(earlier * hit_first, 0, keepdims=True).astype(i32)
    slot_second = jnp.sum(earlier * hit_second, 0, keepdims=True).astype(i32)
    lines = packed_ref.shape[0]
    height = lines * slots // (experts * capacity)
    place = lax.broadcasted_iota(i32, (lines, row_count), 0)
    row = lax.broadcasted_iota(i32, (lines, row_count), 1)
    plane, inner = place // height, place % height
    routed_place = jnp.where(inner < slots, plane * slots + inner, -1)
    dense_place = jnp.where(
        inner < slots, -1, plane % shared * (height - slots) + inner - slots
    )
    at_first = routed_place == first * capacity + slot_first
    at_second = routed_place == second * capacity + slot_second
    at_row = dense_place == row
    chosen = (at_first | at_second | at_row).astype(jnp.bfloat16)
    packed_ref[...] = jnp.dot(
        chosen, own.astype(jnp.bfloat16), preferred_element_type=f32
    ).astype(jnp.bfloat16)
    factors = (
        jnp.where(at_first, route_weights_ref[0:1, :], 0.0)
        + jnp.where(at_second, route_weights_ref[1:2, :], 0.0)
        + jnp.where(at_row, branch, 0.0)
    )
    factors_ref[...] = factors


def norm_and_pack(
    everyone,
    tokens,
    first_gain,
    branch_gate,
    routes,
    route_weights,
    lines,
    experts,
    capacity,
    slots,
    shared,
):
    row_count, quarter = tokens.shape[0], everyone.shape[2]
    vmem = pl.BlockSpec(memory_space=pltpu.VMEM)
    return pl.pallas_call(
        partial(norm_kernel, experts=experts, capacity=capacity, slots=slots, shared=shared),
        out_shape=(
            pltpu.VMEM((lines, quarter), jnp.bfloat16),
            pltpu.VMEM((row_count, quarter), jnp.float32),
            pltpu.VMEM((lines, row_count), jnp.float32),
        ),
        in_specs=[vmem] * 6,
        out_specs=(vmem, vmem, vmem),
        name="norm_and_pack",
    )(
        on_chip(everyone),
        on_chip(tokens),
        on_chip(first_gain[None]),
        on_chip(branch_gate[None]),
        on_chip(routes.T),
        on_chip(route_weights.T),
    )


def fan_choice(planes, slots_part, capacity, here, splits, shared):
    part = slots_part - here * capacity
    rows = planes * capacity
    index = np.arange(rows + shared * part)
    choice = np.zeros((here, splits, len(index), planes * slots_part), np.float32)
    for e in range(here):
        for i in range(splits):
            dense = index - rows
            routed_from = index // capacity * slots_part + e * capacity + index % capacity
            dense_from = (
                (i * shared + dense // part) * slots_part + here * capacity + dense % part
            )
            choice[e, i, index, np.where(index < rows, routed_from, dense_from)] = 1
    return choice.reshape(here * splits * len(index), planes * slots_part)


def fan_kernel(arrived_ref, choice_ref, out_any, laid_ref, sent):
    planes, slots_part, quarter = arrived_ref.shape
    here, copies, splits, height, _ = out_any.shape
    arrived = arrived_ref[...].reshape(planes * slots_part, quarter)
    for e in range(here):
        size = splits * height
        laid = jnp.dot(
            choice_ref[e * size : (e + 1) * size, :], arrived, preferred_element_type=jnp.float32
        ).astype(jnp.bfloat16)
        for c in range(copies):
            laid_ref[e, c] = laid.reshape(splits, height, quarter)
        pltpu.make_async_copy(laid_ref.at[e], out_any.at[e], sent.at[0]).start()
    pltpu.make_async_copy(laid_ref, out_any, sent.at[0]).wait()


def fan_out(arrived, capacity, here, copies, splits, shared):
    planes, slots_part, quarter = arrived.shape
    choice = fan_choice(planes, slots_part, capacity, here, splits, shared)
    height = choice.shape[0] // (here * splits)
    vmem = pl.BlockSpec(memory_space=pltpu.VMEM)
    shape = (here, copies, splits, height, quarter)
    return pl.pallas_call(
        fan_kernel,
        out_shape=jax.ShapeDtypeStruct(shape, jnp.bfloat16),
        in_specs=[vmem, vmem],
        out_specs=pl.BlockSpec(memory_space=pl.ANY),
        scratch_shapes=[pltpu.VMEM(shape, jnp.bfloat16), pltpu.SemaphoreType.DMA((1,))],
        name="fan_out",
    )(on_chip(arrived), on_chip(jnp.asarray(choice, jnp.bfloat16)))


def gather_kernel(returned_ref, out_ref, *, capacity, here, splits, shared):
    planes, slots_part, quarter = out_ref.shape
    sources, height, _ = returned_ref.shape
    part = slots_part - here * capacity
    rows = planes * capacity
    f32 = jnp.float32
    routed = []
    for e in range(here):
        total = jnp.zeros((rows, quarter), f32)
        for s in range(e * (sources // here), (e + 1) * (sources // here)):
            total = total + returned_ref[s, :rows, :].astype(f32)
        routed.append(total)
    dense = []
    for i in range(splits):
        total = jnp.zeros((height - rows, quarter), f32)
        for s in range(i, sources, splits):
            total = total + returned_ref[s, rows:, :].astype(f32)
        dense.append(total)
    sums = jnp.concatenate(routed + dense, 0).astype(jnp.bfloat16)
    shape = (planes * slots_part, sums.shape[0])
    line = lax.broadcasted_iota(jnp.int32, shape, 0)
    column = lax.broadcasted_iota(jnp.int32, shape, 1)
    z, inner = line // slots_part, line % slots_part
    routed_from = inner // capacity * rows + z * capacity + inner % capacity
    dense_from = here * rows + z * part + inner - here * capacity
    chosen = (
        column == jnp.where(inner < here * capacity, routed_from, dense_from)
    ).astype(jnp.bfloat16)
    laid = jnp.dot(chosen, sums, preferred_element_type=f32).astype(jnp.bfloat16)
    out_ref[...] = laid.reshape(planes, slots_part, quarter)


def gather_back(returned, planes, slots_part, capacity, here, splits, shared):
    vmem = pl.BlockSpec(memory_space=pltpu.VMEM)
    return pl.pallas_call(
        partial(gather_kernel, capacity=capacity, here=here, splits=splits, shared=shared),
        out_shape=pltpu.VMEM((planes, slots_part, returned.shape[2]), jnp.bfloat16),
        in_specs=[vmem],
        out_specs=vmem,
        name="gather_back",
    )(on_chip(returned))


def first_norm(values, gain):
    centre = jnp.mean(values, -1, keepdims=True)
    spread = jnp.mean(jnp.square(values - centre), -1, keepdims=True)
    return ((values - centre) * lax.rsqrt(spread + norm_epsilon) * gain).astype(jnp.bfloat16)


def shards(
    tokens,
    state,
    w_recep,
    w_key,
    w_value,
    w_out,
    decay_base,
    decay_down,
    decay_up,
    rate_base,
    rate_down,
    rate_up,
    head_gain,
    first_gain,
    expert_gate,
    expert_up,
    expert_down,
    dense_gate,
    dense_up,
    dense_down,
    branch_gate,
    second_gain,
    routes,
    route_weights,
):
    row_count = tokens.shape[0]
    model_width = tokens.shape[1]
    quarter = w_recep.shape[1]
    planes = lax.axis_size("z")
    plane_blocks = lax.axis_size(("x", "c"))
    plane_size = lax.axis_size(PLANE)
    tp_size = lax.axis_size("tp")
    shared = planes // tp_size
    message = mixer_message(
        tp_size,
        dense_down,
        tokens,
        state,
        w_recep,
        w_key,
        w_value,
        w_out,
        decay_base,
        decay_down,
        decay_up,
        rate_base,
        rate_down,
        rate_up,
        head_gain,
    )
    everyone = exchange(message, "tp")
    everyone, dense_gate, dense_up, branch_gate, expert_gate, expert_up, expert_down = (
        lax.optimization_barrier(
            (everyone, dense_gate, dense_up, branch_gate, expert_gate, expert_up, expert_down)
        )
    )
    mix_rows = tp_size * row_count
    units = jnp.concatenate(
        [padded_units(dense_gate, 8), padded_units(dense_up, 8)]
        + [everyone[i, mix_rows:] for i in range(tp_size)],
        1,
    )
    units = with_neighbour(units, 2)
    units = with_neighbour(units, 1)
    experts = lax.axis_size(EP) // SPLIT
    here = experts // planes
    capacity = min(row_count, max(2, 2 * row_count * routes.shape[1] // experts))
    slots = here * capacity
    part = row_count // shared
    packed_rows, own_columns, factors = norm_and_pack(
        everyone,
        tokens,
        first_gain,
        branch_gate,
        routes,
        route_weights,
        planes * (slots + part),
        experts,
        capacity,
        slots,
        shared,
    )
    arrived = exchange(packed_rows.reshape(planes, slots + part, quarter), "z")
    rows = planes * capacity
    dense_count = shared * part
    height = rows + dense_count
    outgoing = fan_out(arrived, capacity, here, plane_blocks // here, tp_size, shared)
    everything = exchange(outgoing.reshape(plane_size, height, quarter), PLANE)
    everything = everything.reshape(plane_blocks, tp_size, height, quarter)
    returning = run_experts(
        everything, units, expert_gate[0], expert_up[0], expert_down[0], rows
    )
    returned = exchange(returning.reshape(plane_size, height, quarter), PLANE)
    back = gather_back(returned, planes, slots + part, capacity, here, tp_size, shared)
    back = exchange(back, "z").reshape(planes * (slots + part), quarter)
    second_sum = residual_scale * own_columns + lax.dot_general(
        factors,
        back.astype(jnp.float32),
        (((0,), (0,)), ((), ())),
        precision=lax.Precision.HIGHEST,
        preferred_element_type=jnp.float32,
    )
    row_sums, square_sums = in_one(
        (jnp.sum(second_sum, 1), jnp.sum(second_sum * second_sum, 1)), "tp"
    )
    average = row_sums / model_width
    spread = square_sums / model_width - average * average
    return (
        (second_sum - average[:, None]) * lax.rsqrt(spread + norm_epsilon)[:, None] * second_gain
    ).astype(jnp.bfloat16)


def solution(mesh):
    finer = Mesh(mesh.devices.reshape(16, 4, 2, mesh.shape["tp"]), ("z", "x", "c", "tp"))
    return jax.shard_map(
        shards,
        mesh=finer,
        in_specs=(
            P(EP, None),
            P(EP, "tp", None, None),
            P(None, "tp"),
            P(None, "tp"),
            P(None, "tp"),
            P("tp", None),
            P("tp"),
            P(),
            P(None, "tp"),
            P("tp"),
            P(),
            P(None, "tp"),
            P("tp"),
            P(),
            P(EP, None, "tp"),
            P(EP, None, "tp"),
            P(EP, "tp", None),
            P(EP, None),
            P(EP, None),
            P(EP, "tp"),
            P(),
            P("tp"),
            P(EP, None),
            P(EP, None),
        ),
        out_specs=P(EP, "tp"),
        check_vma=False,
    )
```
